32 devices in a mesh: sp: 8 (over z, y), tp: 4 (over x, core).
Axes of the slice: x: 2, y: 2, z: 4, core: 2. Of those that a mesh axis runs over, the one named last changes fastest.
Arguments:
- block_input: bfloat16 [8192, 2048], P('sp'), may hold values from -6 to 6
- out_grad: bfloat16 [8192, 2048], P('sp'), may hold values from -6 to 6
- w_value: bfloat16 [2048, 1024], P(None, 'tp'), may hold values from -0.125 to 0.125
- w_gate: bfloat16 [2048, 1024], P(None, 'tp'), may hold values from -0.125 to 0.125
- conv_taps: float32 [31, 1024], P(None, 'tp'), may hold values from -4 to 4
- norm_gain: float32 [1024], P('tp'), may hold values from 0.1 to 1.9
- norm_shift: float32 [1024], P('tp'), may hold values from -3 to 3
- w_proj: bfloat16 [1024, 2048], P('tp'), may hold values from -0.1875 to 0.1875
Outputs:
- input_grad: bfloat16 [8192, 2048], P('sp', 'tp')
- value_wgrad: float32 [2048, 1024], P('sp', 'tp')
- gate_wgrad: float32 [2048, 1024], P('sp', 'tp')
- proj_wgrad: float32 [1024, 2048], P('tp', 'sp')
- taps_grad: float32 [31, 1024], P(None, 'tp')
- gain_grad: float32 [1024], P('tp')
- shift_grad: float32 [1024], P('tp')
The draws below stay inside these ranges and needn't reach their ends.
All inputs are finite; a program needn't handle non-finite values.
Results may differ from the reference program's by a relative error of at most 0.014.
Values may be sent and summed in bfloat16 or wider, within the bound.
A program may use at most 128 MiB of HBM per device.

```python
import math
import jax
import jax.numpy as jnp
from jax import lax

D = 2048
CH = 1024
KERNEL = 31
TOKENS = 8192
N_TP = 4


def draw_conv_taps(key, part):
    base = jax.random.fold_in(key, 11)
    first, second, third = jax.random.split(base, 3)
    channel = jnp.arange(CH, dtype=jnp.float32)
    phase = jax.random.uniform(first, (), jnp.float32, 0.0, 6.2831)
    level = jnp.exp(1.2 * jnp.sin(6.2831853 * channel / CH + phase))
    rough = jnp.exp(jax.random.uniform(second, (CH,), jnp.float32, -0.7, 0.7))
    taps = jax.random.truncated_normal(third, -3.0, 3.0, (KERNEL, CH), jnp.float32)
    return (taps * (level * rough)[None, :] / math.sqrt(KERNEL)).astype(jnp.float32)


def with_spikes(entries, rng, source, target, parts, factor):
    def block_of(dim):
        return (jnp.arange(entries.shape[dim]) // (entries.shape[dim] // parts)).reshape((-1,) + (1,) * (entries.ndim - 1 - dim))

    one_side = jax.random.permutation(rng, parts)[block_of(target)]
    other_side = (block_of(target) + parts // 2) % parts
    return jnp.where((block_of(source) == one_side) | (block_of(source) == other_side), factor * entries, entries)


def shard_levels(rng, dims, cuts, low, top_value):
    def one(dim, shards_of):
        steps = jax.random.uniform(jax.random.fold_in(jax.random.fold_in(rng, 6), dim), (shards_of,), jnp.float32, low / len(cuts), top_value / len(cuts))
        return jnp.repeat(jnp.exp(steps), dims[dim] // shards_of).reshape((-1,) + (1,) * (len(dims) - dim - 1))

    gain = one(*cuts[0])
    for cut in cuts[1:]:
        gain = gain * one(*cut)
    return gain


def scatter_about(stream_key, dims, spread, reach, pieces=(), kind=jnp.bfloat16):
    result = spread * jax.random.normal(stream_key, dims, jnp.float32)
    if pieces:
        result = result * shard_levels(stream_key, dims, pieces, -0.22, 0.18)
    return jnp.clip(result, -reach, reach).astype(kind)


def gaussian_with(own_key, dims, scale, limit, cuts, heavy, kind=jnp.bfloat16):
    entries = scale * jax.random.normal(own_key, dims, jnp.float32)
    if cuts:
        entries = entries * shard_levels(own_key, dims, cuts, -0.22, 0.18)
    return jnp.clip(with_spikes(entries, jax.random.fold_in(own_key, 3), *heavy), -limit, limit).astype(kind)


def setup_inputs(seed: int = 0) -> dict:
    streams_of = jax.random.split(jax.random.key(seed), 9)
    block_input = scatter_about(streams_of[0], (TOKENS, D), 1.0, 6.0, ((0, 8),))
    out_grad = gaussian_with(streams_of[1], (TOKENS, D), 1.0, 6.0, ((0, 8),), (0, 1, 8, 2.0))
    w_value = scatter_about(streams_of[2], (D, CH), D ** -0.5, 0.125, ((1, 4),))
    w_gate = scatter_about(streams_of[3], (D, CH), D ** -0.5, 0.125, ((1, 4),))
    conv_taps = draw_conv_taps(jax.random.fold_in(streams_of[8], 71), 0)
    norm_gain = jnp.clip(1.0 + 0.18 * jax.random.normal(streams_of[5], (CH,), jnp.float32), 0.1, 1.9)
    norm_shift = scatter_about(streams_of[6], (CH,), 0.5, 3.0, ((0, 4),), jnp.float32)
    w_proj = scatter_about(streams_of[7], (CH, D), CH ** -0.5, 0.1875, ((0, 4),))
    return {"block_input": block_input, "out_grad": out_grad, "w_value": w_value, "w_gate": w_gate, "conv_taps": conv_taps, "norm_gain": norm_gain, "norm_shift": norm_shift, "w_proj": w_proj}


EPS = 0.05

def reference(block_input, out_grad, w_value, w_gate, conv_taps, norm_gain, norm_shift, w_proj):
    value_proj = jnp.dot(block_input, w_value, preferred_element_type=jnp.float32).astype(jnp.bfloat16)
    gate_proj = jnp.dot(block_input, w_gate, preferred_element_type=jnp.float32).astype(jnp.bfloat16)
    gate_sigmoid = jax.nn.sigmoid(gate_proj.astype(jnp.float32))
    value_wide = value_proj.astype(jnp.float32)
    gated_input = (value_wide * gate_sigmoid).astype(jnp.bfloat16)
    padded_glu = jnp.pad(gated_input.astype(jnp.float32), ((KERNEL - 1, 0), (0, 0)))
    filtered = jnp.zeros((TOKENS, CH), jnp.float32)
    for tap_index in range(KERNEL):
        begin = KERNEL - 1 - tap_index
        filtered = filtered + conv_taps[tap_index] * padded_glu[begin:begin + TOKENS]
    row_mean = lax.optimization_barrier(jnp.sum(filtered, axis=1)) / CH
    row_var = lax.optimization_barrier(jnp.sum(filtered * filtered, axis=1)) / CH - row_mean * row_mean
    row_scale = lax.rsqrt(row_var + EPS)
    normed = (filtered - row_mean[:, None]) * row_scale[:, None]
    activated = normed * norm_gain + norm_shift
    act_sigmoid = jax.nn.sigmoid(activated)
    mixer_out = (activated * act_sigmoid).astype(jnp.bfloat16)
    grad_mixed = jnp.dot(out_grad, w_proj.T, preferred_element_type=jnp.float32)
    grad_act = grad_mixed * act_sigmoid * (1.0 + activated * (1.0 - act_sigmoid))
    grad_normed = grad_act * norm_gain
    first_mean = lax.optimization_barrier(jnp.sum(grad_normed, axis=1)) / CH
    second_mean = lax.optimization_barrier(jnp.sum(grad_normed * normed, axis=1)) / CH
    grad_filtered = row_scale[:, None] * (grad_normed - first_mean[:, None] - normed * second_mean[:, None])
    padded_grad = jnp.pad(grad_filtered, ((0, KERNEL - 1), (0, 0)))
    grad_glu = jnp.zeros((TOKENS, CH), jnp.float32)
    taps_rows = []
    for tap_index in range(KERNEL):
        begin = KERNEL - 1 - tap_index
        grad_glu = grad_glu + conv_taps[tap_index] * padded_grad[tap_index:tap_index + TOKENS]
        taps_rows.append(lax.optimization_barrier(jnp.sum(grad_filtered * padded_glu[begin:begin + TOKENS], axis=0)))
    grad_value = (grad_glu * gate_sigmoid).astype(jnp.bfloat16)
    grad_gate = (grad_glu * value_wide * gate_sigmoid * (1.0 - gate_sigmoid)).astype(jnp.bfloat16)
    block_cols = CH // N_TP
    summed = jnp.zeros((TOKENS, D), jnp.float32)
    for block_index in range(N_TP):
        low = block_index * block_cols
        high = low + block_cols
        partial_sum = jnp.dot(grad_value[:, low:high], w_value[:, low:high].T, preferred_element_type=jnp.float32)
        partial_sum = partial_sum + jnp.dot(grad_gate[:, low:high], w_gate[:, low:high].T, preferred_element_type=jnp.float32)
        summed = summed + partial_sum.astype(jnp.bfloat16).astype(jnp.float32)
    input_grad = summed.astype(jnp.bfloat16)
    loss_scale = 1.0 / jnp.sqrt(jnp.float32(TOKENS))
    value_wgrad = jnp.dot(block_input.T, grad_value, preferred_element_type=jnp.float32) * loss_scale
    gate_wgrad = jnp.dot(block_input.T, grad_gate, preferred_element_type=jnp.float32) * loss_scale
    proj_wgrad = jnp.dot(mixer_out.T, out_grad, preferred_element_type=jnp.float32) * loss_scale
    taps_grad = jnp.stack(taps_rows, axis=0) * loss_scale
    gain_grad = lax.optimization_barrier(jnp.sum(grad_act * normed, axis=0)) * loss_scale
    shift_grad = lax.optimization_barrier(jnp.sum(grad_act, axis=0)) * loss_scale
    return (input_grad, value_wgrad, gate_wgrad, proj_wgrad, taps_grad, gain_grad, shift_grad)
```

```python
import functools
import math

import jax
import jax.numpy as jnp
from jax import lax
from jax.experimental import pallas as pl
from jax.experimental.pallas import tpu as pltpu
from jax.sharding import PartitionSpec as P

EPS = 0.05
MESH = pl.DeviceIdType.MESH
LANES = 128
BF, F32 = jnp.bfloat16, jnp.float32


def right_product(left, right):
    return lax.dot_general(
        left, right, (((1,), (1,)), ((), ())), preferred_element_type=F32
    )


def column_product(left, right):
    return lax.dot_general(
        left, right, (((0,), (0,)), ((), ())), preferred_element_type=F32
    )


def main_kernel(
    n, n_tp, n_chan, halo,
    bi_hbm, og_hbm, wv_hbm, wg_hbm, wp_hbm, taps_ref, gain_ref, shift_ref,
    ig_ref, ws_ref, ps_ref, sm_ref,
    bi, og, wv, wg, wp,
    gx, vp, sg, fl, nm, gn, gf, gm, mo, gb, tacc, cols, rowbuf, so, si,
    gs, gr, gs2, gq, pm, pr, pm2, pq,
    xs, xr, ys, yr, acc, small, small_pair, small_in, small_all,
    load_sem, st_send, st_recv, hx_send, hx_recv, hf_send, hf_recv,
    gs_send, gs_recv, gq_send, gq_recv, pr_send, pr_recv, pq_send, pq_recv,
    x_send, x_recv, y_send, y_recv, s_send, s_recv, sa_send, sa_recv,
):
    me, t = lax.axis_index("sp"), lax.axis_index("tp")
    outer, inner = me // 2, me % 2
    h = n // 2
    mate = 2 * outer + (1 - inner)
    t_near, t_far = t + 1 - 2 * (t % 2), lax.rem(t + n_tp // 2, n_tp)
    t_cross = lax.rem(t_near + n_tp // 2, n_tp)
    tokens, width = bi.shape
    rows, cols_tp = width // n, width // n_tp
    chans = wv.shape[1]
    halves = chans // LANES
    kernel_len = taps_ref.shape[0]
    chunks = xs.shape[0]
    step = tokens // chunks
    block = 64
    per = step // block

    def load(src, dst, i):
        copy = pltpu.make_async_copy(src, dst, load_sem.at[i])
        copy.start()
        return copy

    def piece(r):
        return pl.ds(r * step, step)

    order_in = [chunks - 1] + list(range(chunks - 1))
    load_w = [load(wv_hbm, wv, 0), load(wg_hbm, wg, 1)]
    load_bi = {r: load(bi_hbm.at[piece(r)], bi.at[piece(r)], 3 + r) for r in order_in}
    load_wp = load(wp_hbm, wp, 2)
    load_og = [load(og_hbm.at[piece(r)], og.at[piece(r)], 3 + chunks + r) for r in range(chunks)]

    barrier = pltpu.get_barrier_semaphore()
    peers = [{"sp": 2 * lax.rem(outer + k, h) + inner} for k in range(1, h)]
    peers += [{"sp": mate}, {"sp": lax.rem(me + 1, n)}, {"sp": lax.rem(me + n - 1, n)}]
    peers += [{"tp": lax.rem(t + k, n_tp)} for k in range(1, n_tp)]
    for who in peers:
        pl.semaphore_signal(barrier, inc=1, device_id=who, device_id_type=MESH)

    first, last = me == 0, me == n - 1
    tacc[...] = jnp.zeros_like(tacc)

    @pl.when(first)
    def _():
        gx[:, :halo, :] = jnp.zeros((halves, halo, LANES), F32)

    @pl.when(last)
    def _():
        gf[:, tokens:, :] = jnp.zeros((halves, halo, LANES), F32)

    pl.semaphore_wait(barrier, len(peers))

    def describe(src, dst, send_sem, recv_sem, who):
        return pltpu.make_async_remote_copy(
            src_ref=src, dst_ref=dst, send_sem=send_sem, recv_sem=recv_sem,
            device_id=who, device_id_type=MESH,
        )

    def send(*args):
        copy = describe(*args)
        copy.start()
        return copy

    sent = []

    halo_x = describe(
        gx.at[:, pl.ds(tokens, halo), :], gx.at[:, pl.ds(0, halo), :],
        hx_send.at[0], hx_recv.at[0], {"sp": lax.rem(me + 1, n)},
    )
    for copy in load_w:
        copy.wait()
    for r in order_in:
        load_bi[r].wait()
        where = piece(r)
        value = jnp.dot(bi[where, :], wv[...], preferred_element_type=F32).astype(BF)
        gate = jnp.dot(bi[where, :], wg[...], preferred_element_type=F32).astype(BF).astype(F32)
        sigmoid = jax.nn.sigmoid(gate)
        gated = (value.astype(F32) * sigmoid).astype(BF).astype(F32)
        vp[where, :] = value
        sg[where, :] = sigmoid
        for c in range(halves):
            gx[c, pl.ds(halo + r * step, step), :] = gated[:, c * LANES:(c + 1) * LANES]
        if r == chunks - 1:
            @pl.when(me < n - 1)
            def _():
                halo_x.start()

    @pl.when(me > 0)
    def _():
        halo_x.wait_recv()

    lane = lax.broadcasted_iota(jnp.int32, (block, LANES), 1)

    def send_stats(phase, r):
        so[phase, r] = rowbuf[...].T[:8]
        copies = [
            send(so.at[phase, r], si.at[phase, r, k - 1], st_send.at[phase, r, k - 1],
                 st_recv.at[phase, r, k - 1], {"tp": lax.rem(t + k, n_tp)})
            for k in range(1, n_tp)
        ]
        sent.extend(copies)
        return copies

    def take_stats(phase, r, copies):
        total = so[phase, r]
        for k, copy in enumerate(copies):
            copy.wait_recv()
            total = total + si[phase, r, k]
        return total / n_chan

    def rows_of(base, i):
        return pl.ds(pl.multiple_of(base + i * block, block), block)

    def pair_of_sums(i, first_sum, second_sum):
        rowbuf[rows_of(0, i), :] = jnp.where(
            lane == 0, first_sum, jnp.where(lane == 1, second_sum, 0.0)
        )

    def conv_chunk(r):
        def body(i, carry):
            sums = jnp.zeros((block, LANES), F32)
            squares = jnp.zeros((block, LANES), F32)
            for c in range(halves):
                total = jnp.zeros((block, LANES), F32)
                for k in range(kernel_len):
                    where = pl.ds(r * step + i * block + halo - k, block)
                    total = total + taps_ref[pl.ds(k, 1), c * LANES:(c + 1) * LANES] * gx[c, where, :]
                fl[c, rows_of(r * step, i), :] = total
                sums = sums + total
                squares = squares + total * total
            pair_of_sums(i, jnp.sum(sums, axis=1, keepdims=True), jnp.sum(squares, axis=1, keepdims=True))
            return carry

        lax.fori_loop(0, per, body, 0)
        return send_stats(0, r)

    moments = [conv_chunk(r) for r in range(chunks)]

    load_wp.wait()

    def norm_chunk(r, carry):
        load_og[r].wait()
        gm[...] = right_product(og[piece(r), :], wp[...])
        total = take_stats(0, r, moments[r])
        mean = total[0:1]
        scale = lax.rsqrt(total[1:2] - mean * mean + EPS)
        both = jnp.where(lax.broadcasted_iota(jnp.int32, total.shape, 0) == 0, mean, scale)
        cols[0, piece(r), :8] = both.T

        def body(i, carry):
            where = rows_of(r * step, i)
            mean = cols[0, where, 0:1]
            scale = cols[0, where, 1:2]
            sums = jnp.zeros((block, LANES), F32)
            crosses = jnp.zeros((block, LANES), F32)
            out = []
            for c in range(halves):
                at = slice(c * LANES, (c + 1) * LANES)
                gain, shift = gain_ref[:, at], shift_ref[:, at]
                normed = (fl[c, where, :] - mean) * scale
                activated = normed * gain + shift
                sigmoid = jax.nn.sigmoid(activated)
                mo[where, at] = (activated * sigmoid).astype(BF)
                grad_act = gm[rows_of(0, i), at] * sigmoid * (1.0 + activated * (1.0 - sigmoid))
                grad_normed = grad_act * gain
                nm[c, where, :] = normed
                gn[c, where, :] = grad_normed
                sums = sums + grad_normed
                crosses = crosses + grad_normed * normed
                fold = lambda x: x.reshape(block // 8, 8, LANES).sum(axis=0)
                out.append(carry[2 * c] + fold(grad_act * normed))
                out.append(carry[2 * c + 1] + fold(grad_act))
            pair_of_sums(i, jnp.sum(sums, axis=1, keepdims=True), jnp.sum(crosses, axis=1, keepdims=True))
            return tuple(out)

        carry = lax.fori_loop(0, per, body, carry)
        return send_stats(1, r), carry

    carry = tuple(jnp.zeros((8, LANES), F32) for _ in range(2 * halves))
    means = []
    for r in range(chunks):
        copies, carry = norm_chunk(r, carry)
        means.append(copies)
    small[...] = jnp.zeros_like(small)
    for c in range(halves):
        at = slice(c * LANES, (c + 1) * LANES)
        small[kernel_len:kernel_len + 1, at] = carry[2 * c].sum(axis=0, keepdims=True)
        small[kernel_len + 1:kernel_len + 2, at] = carry[2 * c + 1].sum(axis=0, keepdims=True)

    aligned = rows % LANES == 0
    wide = 256
    order = [lax.rem(outer + k, h) for k in range(1, h)] + [outer]

    def block_rows(o, i):
        return pl.ds(pl.multiple_of((2 * o + i) * rows, rows), rows)

    def make_block(store, act, other, o, i):
        if aligned:
            where = block_rows(o, i)
            store[where, :] = column_product(act[:, where], other[...]).astype(BF)

    def make_all(store, act, other):
        if not aligned:
            for c in range(width // wide):
                where = pl.ds(c * wide, wide)
                store[where, :] = column_product(act[:, where], other[...]).astype(BF)

    def mate_block(store, act, other, landing, send_sem, recv_sem, k):
        make_block(store, act, other, order[k], 1 - inner)
        where = block_rows(order[k], 1 - inner)
        return send(store.at[where], landing.at[k], send_sem.at[k], recv_sem.at[k], {"sp": mate})

    def outer_block(store, act, other, landing, copies, second, landed, send_sem, recv_sem, k):
        make_block(store, act, other, order[k], inner)
        copies[k].wait_recv()
        total = store[block_rows(order[k], inner), :].astype(F32) + landing[k].astype(F32)
        if k == h - 1:
            return total
        second[k] = total.astype(BF)
        return send(second.at[k], landed.at[k], send_sem.at[k], recv_sem.at[k], {"sp": 2 * order[k] + inner})

    make_all(pm, og, mo)
    p_copies = [mate_block(pm, og, mo, pr, pr_send, pr_recv, k) for k in range(h)]
    p_outer = []

    def proj_outer(k):
        p_outer.append(outer_block(pm, og, mo, pr, p_copies, pm2, pq, pq_send, pq_recv, k))

    halo_f = describe(
        gf.at[:, pl.ds(0, halo), :], gf.at[:, pl.ds(tokens, halo), :],
        hf_send.at[0], hf_recv.at[0], {"sp": lax.rem(me + n - 1, n)},
    )

    def filtered_chunk(r):
        cols[1, piece(r), :8] = take_stats(1, r, means[r]).T

        def body(i, carry):
            where = rows_of(r * step, i)
            scale = cols[0, where, 1:2]
            first_mean = cols[1, where, 0:1]
            second_mean = cols[1, where, 1:2]
            for c in range(halves):
                gf[c, where, :] = scale * (
                    gn[c, where, :] - first_mean - nm[c, where, :] * second_mean
                )
            return carry

        lax.fori_loop(0, per, body, 0)

    def back_chunk(r):
        def body(i, carry):
            where = rows_of(r * step, i)
            for c in range(halves):
                at = slice(c * LANES, (c + 1) * LANES)
                gated = gx[c, pl.ds(pl.multiple_of(r * step + i * block + halo, 32), block), :]
                total = jnp.zeros((block, LANES), F32)
                for k in range(kernel_len):
                    grad = gf[c, pl.ds(r * step + i * block + k, block), :]
                    total = total + taps_ref[pl.ds(k, 1), at] * grad
                    tacc[c, k] += (gated * grad).reshape(block // 8, 8, LANES).sum(axis=0)
                sigmoid = sg[where, at]
                value = vp[where, at].astype(F32)
                gb[where, at] = (total * sigmoid).astype(BF)
                gb[where, chans + c * LANES:chans + (c + 1) * LANES] = (
                    total * value * sigmoid * (1.0 - sigmoid)
                ).astype(BF)
            return carry

        lax.fori_loop(0, per, body, 0)

    def partial_input(r, j):
        at = pl.ds(pl.multiple_of(j * cols_tp, cols_tp), cols_tp)
        return right_product(gb[piece(r), :chans], wv[at, :]) + right_product(
            gb[piece(r), chans:], wg[at, :]
        )

    x_copies, y_copies = [], []

    def near_block(r):
        xs[r, 0] = partial_input(r, t_cross).astype(BF)
        xs[r, 1] = partial_input(r, t_near).astype(BF)
        x_copies.append(send(xs.at[r], xr.at[r], x_send.at[r], x_recv.at[r], {"tp": t_near}))

    def far_block(r):
        far = partial_input(r, t_far)
        x_copies[r].wait_recv()
        ys[r] = (far + xr[r, 0].astype(F32)).astype(BF)
        y_copies.append(send(ys.at[r], yr.at[r], y_send.at[r], y_recv.at[r], {"tp": t_far}))
        acc[piece(r), :] = partial_input(r, t) + xr[r, 1].astype(F32)

    filtered_chunk(0)

    @pl.when(me > 0)
    def _():
        halo_f.start()

    stage = 0
    for r in range(chunks):
        if r + 1 < chunks:
            filtered_chunk(r + 1)
        else:
            @pl.when(me < n - 1)
            def _():
                halo_f.wait_recv()
        back_chunk(r)
        near_block(r)
        while stage < h * (r + 1) // chunks:
            proj_outer(stage)
            stage += 1
        if r:
            far_block(r - 1)

    make_all(gs, bi, gb)
    g_copies = [mate_block(gs, bi, gb, gr, gs_send, gs_recv, k) for k in range(h)]
    far_block(chunks - 1)

    for c in range(halves):
        small[:kernel_len, c * LANES:(c + 1) * LANES] = tacc[c].sum(axis=1)
    small_copy = send(small, small_in, s_send.at[0], s_recv.at[0], {"sp": mate})
    g_outer = []
    for k in range(h):
        g_outer.append(outer_block(gs, bi, gb, gr, g_copies, gs2, gq, gq_send, gq_recv, k))
        if k == 0:
            small_copy.wait_recv()
            small_pair[...] = small[...] + small_in[...]
            sa_copies = [
                send(small_pair, small_all.at[outer], sa_send.at[j - 1], sa_recv.at[j - 1],
                     {"sp": 2 * lax.rem(outer + j, h) + inner})
                for j in range(1, h)
            ]

    loss_scale = 1.0 / math.sqrt(tokens * n)
    total = p_outer.pop()
    for k, copy in enumerate(p_outer):
        copy.wait_recv()
        total = total + pq[k].astype(F32)
    ps_ref[...] = total * loss_scale
    for copy in sa_copies:
        copy.wait_recv()
    small_all[outer] = small_pair[...]
    total = small_all[0]
    for k in range(1, h):
        total = total + small_all[k]
    sm_ref[...] = total * loss_scale
    for r in range(chunks):
        y_copies[r].wait_recv()
        ig_ref[piece(r), :] = (acc[piece(r), :] + yr[r].astype(F32)).astype(BF)
    total = g_outer.pop()
    for k, copy in enumerate(g_outer):
        copy.wait_recv()
        total = total + gq[k].astype(F32)
    ws_ref[...] = total * loss_scale

    @pl.when(me < n - 1)
    def _():
        halo_x.wait_send()

    @pl.when(me > 0)
    def _():
        halo_f.wait_send()

    for copy in sent + p_copies + p_outer + x_copies + y_copies + g_copies + g_outer + sa_copies + [small_copy]:
        copy.wait_send()


def finish_kernel(
    ig_ref, ws_ref, ps_ref, sm_ref, ig_out, wv_out, wg_out, wp_out, taps_out, gain_out, shift_out,
    turned, taps, gain, shift, sems,
):
    chans = ps_ref.shape[1]
    kernel_len = taps_out.shape[0]
    copies = []

    def store(src, dst):
        copies.append(pltpu.make_async_copy(src, dst, sems.at[len(copies)]))
        copies[-1].start()

    store(ig_ref, ig_out)
    store(ws_ref.at[:, :chans], wv_out)
    store(ws_ref.at[:, chans:], wg_out)
    taps[...] = sm_ref[:kernel_len]
    gain[...] = sm_ref[kernel_len:kernel_len + 1]
    shift[...] = sm_ref[kernel_len + 1:kernel_len + 2]
    store(taps, taps_out)
    store(gain, gain_out)
    store(shift, shift_out)
    turned[...] = ps_ref[...].T
    store(turned, wp_out)
    for copy in copies:
        copy.wait()


def shards(block_input, out_grad, w_value, w_gate, conv_taps, norm_gain, norm_shift, w_proj):
    n, n_tp = lax.axis_size("sp"), lax.axis_size("tp")
    tokens, width = block_input.shape
    chans = w_value.shape[1]
    kernel_len = conv_taps.shape[0]
    halves = chans // LANES
    halo = -(-(kernel_len - 1) // 8) * 8
    rows, cols, h, chunks = width // n, width // n_tp, n // 2, 4
    step = tokens // chunks
    smalls = (-(-(kernel_len + 2) // 8) * 8, chans)
    anywhere = pl.BlockSpec(memory_space=pl.ANY)
    vmem = pl.BlockSpec(memory_space=pltpu.VMEM)
    dma = pltpu.SemaphoreType.DMA
    V = pltpu.VMEM
    shape = jax.ShapeDtypeStruct
    results = pl.pallas_call(
        functools.partial(main_kernel, n, n_tp, chans * n_tp, halo),
        out_shape=(
            shape((tokens, cols), BF), shape((rows, 2 * chans), F32),
            shape((rows, chans), F32), shape(smalls, F32),
        ),
        in_specs=[anywhere] * 5 + [vmem] * 3,
        out_specs=(vmem,) * 4,
        scratch_shapes=[
            V((tokens, width), BF), V((tokens, width), BF), V((width, chans), BF), V((width, chans), BF),
            V((chans, width), BF),
            V((halves, halo + tokens, LANES), F32), V((tokens, chans), BF), V((tokens, chans), F32),
            V((halves, tokens, LANES), F32), V((halves, tokens, LANES), F32), V((halves, tokens, LANES), F32),
            V((halves, tokens + halo, LANES), F32), V((step, chans), F32), V((tokens, chans), BF),
            V((tokens, 2 * chans), BF), V((halves, kernel_len, 8, LANES), F32), V((2, tokens, LANES), F32),
            V((step, LANES), F32), V((2, chunks, 8, step), F32), V((2, chunks, n_tp - 1, 8, step), F32),
            V((width, 2 * chans), BF), V((h, rows, 2 * chans), BF), V((h - 1, rows, 2 * chans), BF),
            V((h - 1, rows, 2 * chans), BF),
            V((width, chans), BF), V((h, rows, chans), BF), V((h - 1, rows, chans), BF),
            V((h - 1, rows, chans), BF),
            V((chunks, 2, step, cols), BF), V((chunks, 2, step, cols), BF), V((chunks, step, cols), BF),
            V((chunks, step, cols), BF), V((tokens, cols), F32),
            V(smalls, F32), V(smalls, F32), V(smalls, F32), V((h,) + smalls, F32),
            dma((3 + 2 * chunks,)), dma((2, chunks, n_tp - 1)), dma((2, chunks, n_tp - 1)),
            dma((1,)), dma((1,)), dma((1,)), dma((1,)),
            dma((h,)), dma((h,)), dma((h - 1,)), dma((h - 1,)), dma((h,)), dma((h,)), dma((h - 1,)), dma((h - 1,)),
            dma((chunks,)), dma((chunks,)), dma((chunks,)), dma((chunks,)), dma((1,)), dma((1,)),
            dma((h - 1,)), dma((h - 1,)),
        ],
        compiler_params=pltpu.CompilerParams(
            collective_id=0, has_side_effects=True, vmem_limit_bytes=56 * 1024 * 1024
        ),
        name="main",
    )(
        block_input, out_grad, w_value, w_gate, w_proj, conv_taps,
        norm_gain.reshape(1, chans), norm_shift.reshape(1, chans),
    )
    outs = pl.pallas_call(
        finish_kernel,
        out_shape=(
            shape((tokens, cols), BF), shape((rows, chans), F32), shape((rows, chans), F32),
            shape((chans, rows), F32), shape((kernel_len, chans), F32), shape((1, chans), F32), shape((1, chans), F32),
        ),
        in_specs=[vmem] * 4,
        out_specs=(anywhere,) * 7,
        scratch_shapes=[
            V((chans, rows), F32), V((kernel_len, chans), F32), V((1, chans), F32), V((1, chans), F32), dma((7,)),
        ],
        name="finish",
    )(*results)
    return outs[:5] + (outs[5].reshape(chans), outs[6].reshape(chans))


def solution(mesh):
    return jax.shard_map(
        shards,
        mesh=mesh,
        in_specs=(
            P("sp", None),
            P("sp", None),
            P(None, "tp"),
            P(None, "tp"),
            P(None, "tp"),
            P("tp"),
            P("tp"),
            P("tp", None),
        ),
        out_specs=(
            P("sp", "tp"),
            P("sp", "tp"),
            P("sp", "tp"),
            P("tp", "sp"),
            P(None, "tp"),
            P("tp"),
            P("tp"),
        ),
        check_vma=False,
    )
```

```python
import functools
import math

import jax
import jax.numpy as jnp
from jax import lax
from jax.experimental import pallas as pl
from jax.experimental.pallas import tpu as pltpu
from jax.sharding import PartitionSpec as P

EPS = 0.05
MESH = pl.DeviceIdType.MESH
LANES = 128
BF, F32 = jnp.bfloat16, jnp.float32


def right_product(left, right):
    return lax.dot_general(
        left, right, (((1,), (1,)), ((), ())), preferred_element_type=F32
    )


def column_product(left, right):
    return lax.dot_general(
        left, right, (((0,), (0,)), ((), ())), preferred_element_type=F32
    )


def main_kernel(
    n, n_tp, n_chan, halo,
    bi_hbm, og_hbm, wv_hbm, wg_hbm, wp_hbm, taps_ref, gain_ref, shift_ref,
    ig_ref, ws_ref, ps_ref, sm_ref,
    bi, og, ww, wp,
    gx, vp, sg, fl, nm, gn, gf, gm, mo, gb, turned, tacc, cols, rowbuf, so, si,
    part, mate_in, low_out, low_in, far_out, far_in,
    xs, xr, ys, yr, acc, small, small_in, small_pair, small_all, small_sum,
    load_sem, st_send, st_recv, hx_send, hx_recv, hf_send, hf_recv,
    mate_send, mate_recv, low_send, low_recv, far_send, far_recv,
    x_send, x_recv, y_send, y_recv, s_send, s_recv, sa_send, sa_recv, sb_send, sb_recv,
):
    me, t = lax.axis_index("sp"), lax.axis_index("tp")
    outer, inner = me // 2, me % 2
    h = n // 2
    mate = 2 * outer + (1 - inner)
    t_near, t_far = t + 1 - 2 * (t % 2), lax.rem(t + n_tp // 2, n_tp)
    t_cross = lax.rem(t_near + n_tp // 2, n_tp)
    tokens, width = bi.shape
    rows, cols_tp = width // n, width // n_tp
    chans, halves = wp.shape[0], ww.shape[0]
    kernel_len = taps_ref.shape[0]
    chunks = xs.shape[0]
    step = tokens // chunks
    block = 64
    per = step // block

    def load(src, dst, i):
        copy = pltpu.make_async_copy(src, dst, load_sem.at[i])
        copy.start()
        return copy

    def piece(r):
        return pl.ds(r * step, step)

    order_in = [chunks - 1] + list(range(chunks - 1))
    load_w = []
    for c in range(halves):
        at = slice(c * LANES, (c + 1) * LANES)
        load_w.append(load(wv_hbm.at[:, at], ww.at[c, :, :LANES], 2 * c))
        load_w.append(load(wg_hbm.at[:, at], ww.at[c, :, LANES:], 2 * c + 1))
    load_bi = {r: load(bi_hbm.at[piece(r)], bi.at[piece(r)], 2 * halves + r) for r in order_in}
    load_wp = load(wp_hbm, wp, 2 * halves + chunks)
    load_og = load(og_hbm, og, 2 * halves + chunks + 1)

    barrier = pltpu.get_barrier_semaphore()
    group = h // 4
    levels = group.bit_length() - 1
    place, low = outer // group, outer % group
    low_flips = [(1 << q) * (1 - 2 * ((low // (1 << q)) % 2)) for q in range(levels)]
    flip_near, flip_far = 1 - 2 * (place % 2), 2 - 4 * (place // 2)
    edge = 1 - (place % 2 + place // 2) % 2
    ends = [
        place + flip_near + edge * flip_far, place + flip_far,
        place + flip_near + (1 - edge) * flip_far, place,
    ]

    def outer_of(spot, mask):
        return spot * group + sum((low_flips[q] for q in range(levels) if mask >> q & 1), low)

    peers = [{"sp": 2 * lax.rem(outer + k, h) + inner} for k in range(1, h)]
    peers += [{"sp": mate}, {"sp": lax.rem(me + 1, n)}, {"sp": lax.rem(me + n - 1, n)}]
    peers += [{"tp": lax.rem(t + k, n_tp)} for k in range(1, n_tp)]
    for who in peers:
        pl.semaphore_signal(barrier, inc=1, device_id=who, device_id_type=MESH)

    first, last = me == 0, me == n - 1
    tacc[...] = jnp.zeros_like(tacc)

    @pl.when(first)
    def _():
        gx[:, :halo, :] = jnp.zeros((halves, halo, LANES), F32)

    @pl.when(last)
    def _():
        gf[:, tokens:, :] = jnp.zeros((halves, halo, LANES), F32)

    def describe(src, dst, send_sem, recv_sem, who):
        return pltpu.make_async_remote_copy(
            src_ref=src, dst_ref=dst, send_sem=send_sem, recv_sem=recv_sem,
            device_id=who, device_id_type=MESH,
        )

    def send(*args):
        copy = describe(*args)
        copy.start()
        return copy

    sent = []

    halo_x = describe(
        gx.at[:, pl.ds(tokens, halo), :], gx.at[:, pl.ds(0, halo), :],
        hx_send.at[0], hx_recv.at[0], {"sp": lax.rem(me + 1, n)},
    )
    for copy in load_w:
        copy.wait()
    for r in order_in:
        load_bi[r].wait()
        where = piece(r)
        for c in range(halves):
            at = slice(c * LANES, (c + 1) * LANES)
            both = jnp.dot(bi[where, :], ww[c], preferred_element_type=F32).astype(BF)
            value = both[:, :LANES]
            sigmoid = jax.nn.sigmoid(both[:, LANES:].astype(F32))
            vp[where, at] = value
            sg[where, at] = sigmoid
            gx[c, pl.ds(halo + r * step, step), :] = (value.astype(F32) * sigmoid).astype(BF).astype(F32)

    pl.semaphore_wait(barrier, len(peers))

    @pl.when(me < n - 1)
    def _():
        halo_x.start()

    load_og.wait()

    lane = lax.broadcasted_iota(jnp.int32, (block, LANES), 1)

    def send_stats(phase, r):
        so[phase, r] = rowbuf[...].T[:8]
        copies = [
            send(so.at[phase, r], si.at[phase, r, k - 1], st_send.at[phase, r, k - 1],
                 st_recv.at[phase, r, k - 1], {"tp": lax.rem(t + k, n_tp)})
            for k in range(1, n_tp)
        ]
        sent.extend(copies)
        return copies

    def take_stats(phase, r, copies):
        total = so[phase, r]
        for k, copy in enumerate(copies):
            copy.wait_recv()
            total = total + si[phase, r, k]
        return total / n_chan

    def rows_of(base, i):
        return pl.ds(pl.multiple_of(base + i * block, block), block)

    def pair_of_sums(i, first_sum, second_sum):
        rowbuf[rows_of(0, i), :] = jnp.where(
            lane == 0, first_sum, jnp.where(lane == 1, second_sum, 0.0)
        )

    def conv_chunk(r):
        def body(i, carry):
            sums = jnp.zeros((block, LANES), F32)
            squares = jnp.zeros((block, LANES), F32)
            for c in range(halves):
                total = jnp.zeros((block, LANES), F32)
                for k in range(kernel_len):
                    where = pl.ds(r * step + i * block + halo - k, block)
                    total = total + taps_ref[pl.ds(k, 1), c * LANES:(c + 1) * LANES] * gx[c, where, :]
                fl[c, rows_of(r * step, i), :] = total
                sums = sums + total
                squares = squares + total * total
            pair_of_sums(i, jnp.sum(sums, axis=1, keepdims=True), jnp.sum(squares, axis=1, keepdims=True))
            return carry

        lax.fori_loop(0, per, body, 0, unroll=2)
        return send_stats(0, r)

    late_first = list(range(1, chunks)) + [0]
    moments, means = {}, {}
    for r in late_first:
        if r == 0:
            @pl.when(me > 0)
            def _():
                halo_x.wait_recv()
        moments[r] = conv_chunk(r)

    def norm_chunk(r):
        total = take_stats(0, r, moments[r])
        mean = total[0:1]
        scale = lax.rsqrt(total[1:2] - mean * mean + EPS)
        both = jnp.where(lax.broadcasted_iota(jnp.int32, total.shape, 0) == 0, mean, scale)
        cols[0, piece(r), :8] = both.T

        def body(i, carry):
            where = rows_of(r * step, i)
            mean = cols[0, where, 0:1]
            scale = cols[0, where, 1:2]
            for c in range(halves):
                at = slice(c * LANES, (c + 1) * LANES)
                normed = (fl[c, where, :] - mean) * scale
                activated = normed * gain_ref[:, at] + shift_ref[:, at]
                sigmoid = jax.nn.sigmoid(activated)
                mo[where, at] = (activated * sigmoid).astype(BF)
                nm[c, where, :] = normed
                fl[c, where, :] = sigmoid
            return carry

        lax.fori_loop(0, per, body, 0, unroll=True)

    def cotangent_chunk(r, carry):
        def body(i, carry):
            where = rows_of(r * step, i)
            sums = jnp.zeros((block, LANES), F32)
            crosses = jnp.zeros((block, LANES), F32)
            out = []
            for c in range(halves):
                at = slice(c * LANES, (c + 1) * LANES)
                gain = gain_ref[:, at]
                normed = nm[c, where, :]
                activated = normed * gain + shift_ref[:, at]
                sigmoid = fl[c, where, :]
                grad_act = gm[where, at] * sigmoid * (1.0 + activated * (1.0 - sigmoid))
                grad_normed = grad_act * gain
                gn[c, where, :] = grad_normed
                sums = sums + grad_normed
                crosses = crosses + grad_normed * normed
                fold = lambda x: x.reshape(block // 8, 8, LANES).sum(axis=0)
                out.append(carry[2 * c] + fold(grad_act * normed))
                out.append(carry[2 * c + 1] + fold(grad_act))
            pair_of_sums(i, jnp.sum(sums, axis=1, keepdims=True), jnp.sum(crosses, axis=1, keepdims=True))
            return tuple(out)

        carry = lax.fori_loop(0, per, body, carry, unroll=True)
        return send_stats(1, r), carry

    for r in late_first:
        norm_chunk(r)

    aligned = rows % LANES == 0
    wide = 256

    blocks_of = [(mask, i) for mask in range(group - 1, -1, -1) for i in range(4)]
    acts = [og] + [bi] * halves
    mate_copies = [[] for _ in acts]
    low_copies = [{} for _ in acts]
    far_copies = [[] for _ in acts]

    def device_block(k, i):
        mask, spot = blocks_of[k]
        return 2 * outer_of(ends[spot], mask) + i

    def make_others(j, other):
        if aligned:
            turned[j] = other.T
        else:
            for w in range(width // wide):
                found = column_product(acts[j][:, w * wide:(w + 1) * wide], other).astype(BF)
                part[j, pl.ds(w * (wide // rows), wide // rows)] = found.reshape(wide // rows, rows, found.shape[1])

    def product(j, b):
        where = pl.ds(pl.multiple_of(b * rows, rows), rows)
        return jnp.dot(turned[j], acts[j][:, where], preferred_element_type=F32)

    def make_mates(j, ks):
        blocks = [device_block(k, 1 - inner) for k in ks]
        if aligned:
            found = [product(j, b) for b in blocks]
            for b, block in zip(blocks, found):
                part[j, b] = block.astype(BF)

    def send_mates(j, ks):
        for k in ks:
            b = device_block(k, 1 - inner)
            mate_copies[j].append(send(
                part.at[j, b], mate_in.at[j, k], mate_send.at[j, k], mate_recv.at[j, k], {"sp": mate}
            ))

    pairs = [range(k, min(k + 2, h)) for k in range(0, h, 2)]

    def mate_blocks(j):
        for ks in pairs:
            make_mates(j, ks)
            send_mates(j, ks)

    def landed(j, slot):
        return describe(
            far_out.at[j, 0], far_in.at[j, slot], far_send.at[j, 0], far_recv.at[j, slot], {"sp": mate}
        )

    def far_step(j, k):
        mask, i = blocks_of[k]
        b = device_block(k, inner)
        total = product(j, b) if aligned else part[j, b].astype(F32)
        mate_copies[j][k].wait_recv()
        total = total + mate_in[j, k].astype(F32)
        lowest = [q for q in range(levels) if mask >> q & 1][:1] or [levels]
        for q in range(lowest[0]):
            came = mask + (1 << q)
            low_copies[j][came, i].wait_recv()
            total = total + low_in[j, (came - 1) * 4 + i].astype(F32)
        if mask:
            at = (mask - 1) * 4 + i
            low_out[j, at] = total.astype(BF)
            low_copies[j][mask, i] = send(
                low_out.at[j, at], low_in.at[j, at], low_send.at[j, at], low_recv.at[j, at],
                {"sp": 2 * outer_of(place, 1 << lowest[0]) + inner},
            )
            return
        if i == 3:
            for slot in (2, 3):
                landed(j, slot).wait_recv()
                total = total + far_in[j, slot].astype(F32)
            return total
        if i:
            @pl.when(edge == 0)
            def _():
                landed(j, i - 1).wait_recv()
                far_out[j, i] = (total + far_in[j, i - 1].astype(F32)).astype(BF)

            @pl.when(edge == 1)
            def _():
                far_out[j, i] = total.astype(BF)

            slot = edge * i + (1 - edge) * 3
            target = edge * (place + flip_near) + (1 - edge) * ends[i]
        else:
            far_out[j, i] = total.astype(BF)
            slot, target = (1 - edge) * 2, place + flip_near
        far_copies[j].append(send(
            far_out.at[j, i], far_in.at[j, slot], far_send.at[j, i], far_recv.at[j, slot],
            {"sp": 2 * outer_of(target, 0) + inner},
        ))

    make_others(0, mo[...])
    make_mates(0, pairs[0])
    send_mates(0, pairs[0])

    load_wp.wait()
    carry = tuple(jnp.zeros((8, LANES), F32) for _ in range(2 * halves))
    for r in range(0, chunks, 2):
        mixed = [right_product(og[piece(i), :], wp[...]) for i in (r, r + 1)]
        gm[piece(r), :] = mixed[0]
        gm[piece(r + 1), :] = mixed[1]
        for i in (r, r + 1):
            means[i], carry = cotangent_chunk(i, carry)
    for ks in pairs[1:]:
        make_mates(0, ks)
    small[...] = jnp.zeros_like(small)
    for c in range(halves):
        small[c, kernel_len:kernel_len + 1] = carry[2 * c].sum(axis=0, keepdims=True)
        small[c, kernel_len + 1:kernel_len + 2] = carry[2 * c + 1].sum(axis=0, keepdims=True)

    halo_f = describe(
        gf.at[:, pl.ds(0, halo), :], gf.at[:, pl.ds(tokens, halo), :],
        hf_send.at[0], hf_recv.at[0], {"sp": lax.rem(me + n - 1, n)},
    )

    def filtered_chunk(r):
        cols[1, piece(r), :8] = take_stats(1, r, means[r]).T

        def body(i, carry):
            where = rows_of(r * step, i)
            scale = cols[0, where, 1:2]
            first_mean = cols[1, where, 0:1]
            second_mean = cols[1, where, 1:2]
            for c in range(halves):
                gf[c, where, :] = scale * (
                    gn[c, where, :] - first_mean - nm[c, where, :] * second_mean
                )
            return carry

        lax.fori_loop(0, per, body, 0, unroll=True)

    def back_chunk(r, c):
        at = slice(c * LANES, (c + 1) * LANES)

        def body(i, carry):
            where = rows_of(r * step, i)
            gated = gx[c, pl.ds(pl.multiple_of(r * step + i * block + halo, 8), block), :]
            total = jnp.zeros((block, LANES), F32)
            for k in range(kernel_len):
                grad = gf[c, pl.ds(r * step + i * block + k, block), :]
                total = total + taps_ref[pl.ds(k, 1), at] * grad
                tacc[c, k] += (gated * grad).reshape(block // 8, 8, LANES).sum(axis=0)
            sigmoid = sg[where, at]
            value = vp[where, at].astype(F32)
            gb[c, where, :LANES] = (total * sigmoid).astype(BF)
            gb[c, where, LANES:] = (total * value * sigmoid * (1.0 - sigmoid)).astype(BF)
            return carry

        lax.fori_loop(0, per, body, 0)

    def partial_input(r, j):
        at = pl.ds(pl.multiple_of(j * cols_tp, cols_tp), cols_tp)
        total = right_product(gb[0, piece(r), :], ww[0, at, :])
        for c in range(1, halves):
            total = total + right_product(gb[c, piece(r), :], ww[c, at, :])
        return total

    x_copies, y_copies = [], []

    def near_block(r):
        xs[r, 0] = partial_input(r, t_cross).astype(BF)
        xs[r, 1] = partial_input(r, t_near).astype(BF)
        x_copies.append(send(xs.at[r], xr.at[r], x_send.at[r], x_recv.at[r], {"tp": t_near}))

    def far_block(r):
        far = partial_input(r, t_far)
        acc[piece(r), :] = partial_input(r, t)
        x_copies[r].wait_recv()
        ys[r] = (far + xr[r, 0].astype(F32)).astype(BF)
        y_copies.append(send(ys.at[r], yr.at[r], y_send.at[r], y_recv.at[r], {"tp": t_far}))
        acc[piece(r), :] += xr[r, 1].astype(F32)

    filtered_chunk(0)

    @pl.when(me > 0)
    def _():
        halo_f.start()

    for ks in pairs[1:]:
        send_mates(0, ks)
    todo = [(j, k) for j in range(1 + halves) for k in range(h - 1)]
    far_step(*todo.pop(0))
    for r in range(1, chunks):
        filtered_chunk(r)


    def far_steps(count):
        for _ in range(count):
            far_step(*todo.pop(0))

    for c in range(halves):
        for r in range(chunks):
            if c == 0 and r == chunks - 1:
                @pl.when(me < n - 1)
                def _():
                    halo_f.wait_recv()
            back_chunk(r, c)
            if c == halves - 1:
                near_block(r)
                if r:
                    far_block(r - 1)
                if r > 1:
                    far_steps(1)
        small[c, :kernel_len] = tacc[c].sum(axis=1)
        if c == halves - 1:
            small_copy = send(small.at[1 - inner], small_in, s_send.at[0], s_recv.at[0], {"sp": mate})
        make_others(1 + c, gb[c])
        mate_blocks(1 + c)
        if c == 0:
            far_steps(1)
    far_block(chunks - 1)

    loss_scale = 1.0 / math.sqrt(tokens * n)
    far_steps(len(todo) - (h - 1))
    small_copy.wait_recv()
    small_pair[...] = small[inner] + small_in[...]
    small_copies = [
        send(small_pair, small_all.at[outer], sa_send.at[k - 1], sa_recv.at[k - 1],
             {"sp": 2 * lax.rem(outer + k, h) + inner})
        for k in range(1, h)
    ]
    far_steps(len(todo) - 1)
    for copy in small_copies:
        copy.wait_recv()
    small_all[outer] = small_pair[...]
    total = small_all[0]
    for k in range(1, h):
        total = total + small_all[k]
    small_sum[inner] = total * loss_scale
    half_copy = send(
        small_sum.at[inner], small_sum.at[inner], sb_send.at[0], sb_recv.at[0], {"sp": mate}
    )
    far_steps(1)

    total = far_step(0, h - 1) * loss_scale
    ps_ref[...] = total if aligned else total.T
    for r in range(chunks):
        y_copies[r].wait_recv()
        ig_ref[piece(r), :] = (acc[piece(r), :] + yr[r].astype(F32)).astype(BF)
    for c in range(halves):
        total = far_step(1 + c, h - 1) * loss_scale
        ws_ref[c] = total.T if aligned else total
    half_copy.wait_recv()
    sm_ref[...] = small_sum[...]

    @pl.when(me < n - 1)
    def _():
        halo_x.wait_send()

    @pl.when(me > 0)
    def _():
        halo_f.wait_send()

    for copies in mate_copies + far_copies + [list(found.values()) for found in low_copies]:
        sent.extend(copies)
    for copy in sent + x_copies + y_copies + small_copies + [small_copy, half_copy]:
        copy.wait_send()


def finish_kernel(
    ig_ref, ws_ref, ps_ref, sm_ref, ig_out, wv_out, wg_out, wp_out, taps_out, gain_out, shift_out,
    taps, gain, shift, sems,
):
    chans = ps_ref.shape[0]
    kernel_len = taps_out.shape[0]
    copies = []

    def store(src, dst):
        copies.append(pltpu.make_async_copy(src, dst, sems.at[len(copies)]))
        copies[-1].start()

    store(ig_ref, ig_out)
    store(ps_ref, wp_out)
    for c in range(chans // LANES):
        at = slice(c * LANES, (c + 1) * LANES)
        store(ws_ref.at[c, :, :LANES], wv_out.at[:, at])
        store(ws_ref.at[c, :, LANES:], wg_out.at[:, at])
        taps[:, at] = sm_ref[c, :kernel_len]
        gain[:, at] = sm_ref[c, kernel_len:kernel_len + 1]
        shift[:, at] = sm_ref[c, kernel_len + 1:kernel_len + 2]
    store(taps, taps_out)
    store(gain, gain_out)
    store(shift, shift_out)
    for copy in copies:
        copy.wait()


def shards(block_input, out_grad, w_value, w_gate, conv_taps, norm_gain, norm_shift, w_proj):
    n, n_tp = lax.axis_size("sp"), lax.axis_size("tp")
    tokens, width = block_input.shape
    chans = w_value.shape[1]
    kernel_len = conv_taps.shape[0]
    halves = chans // LANES
    halo = -(-(kernel_len - 1) // 8) * 8
    rows, cols, h, chunks = width // n, width // n_tp, n // 2, 4
    step = tokens // chunks
    smalls = (-(-(kernel_len + 2) // 8) * 8, LANES)
    pair, sums, lows = 2 * LANES, 1 + halves, max(h - 4, 1)
    part = (pair, rows) if rows % LANES == 0 else (rows, pair)
    anywhere = pl.BlockSpec(memory_space=pl.ANY)
    vmem = pl.BlockSpec(memory_space=pltpu.VMEM)
    dma = pltpu.SemaphoreType.DMA
    V = pltpu.VMEM
    shape = jax.ShapeDtypeStruct
    results = pl.pallas_call(
        functools.partial(main_kernel, n, n_tp, chans * n_tp, halo),
        out_shape=(
            shape((tokens, cols), BF), shape((halves, rows, pair), F32),
            shape((chans, rows), F32), shape((halves,) + smalls, F32),
        ),
        in_specs=[pl.BlockSpec(memory_space=pltpu.HBM)] * 5 + [vmem] * 3,
        out_specs=(vmem,) * 4,
        scratch_shapes=[
            V((tokens, width), BF), V((tokens, width), BF), V((halves, width, pair), BF),
            V((chans, width), BF),
            V((halves, halo + tokens, LANES), F32), V((tokens, chans), BF), V((tokens, chans), F32),
            V((halves, tokens, LANES), F32), V((halves, tokens, LANES), F32), V((halves, tokens, LANES), F32),
            V((halves, tokens + halo, LANES), F32), V((tokens, chans), F32), V((tokens, chans), BF),
            V((halves, tokens, pair), BF), V((sums, pair, tokens), BF), V((halves, kernel_len, 8, LANES), F32), V((2, tokens, LANES), F32),
            V((step, LANES), F32), V((2, chunks, 8, step), F32), V((2, chunks, n_tp - 1, 8, step), F32),
            V((sums, n) + part, BF), V((sums, h) + part, BF), V((sums, lows) + part, BF), V((sums, lows) + part, BF),
            V((sums, 3) + part, BF), V((sums, 4) + part, BF),
            V((chunks, 2, step, cols), BF), V((chunks, 2, step, cols), BF), V((chunks, step, cols), BF),
            V((chunks, step, cols), BF), V((tokens, cols), F32),
            V((halves,) + smalls, F32), V(smalls, F32), V(smalls, F32), V((h,) + smalls, F32),
            V((halves,) + smalls, F32),
            dma((2 * halves + chunks + 2,)), dma((2, chunks, n_tp - 1)), dma((2, chunks, n_tp - 1)),
            dma((1,)), dma((1,)), dma((1,)), dma((1,)),
            dma((sums, h)), dma((sums, h)), dma((sums, lows)), dma((sums, lows)), dma((sums, 3)), dma((sums, 4)),
            dma((chunks,)), dma((chunks,)), dma((chunks,)), dma((chunks,)), dma((1,)), dma((1,)),
            dma((h - 1,)), dma((h - 1,)), dma((1,)), dma((1,)),
        ],
        compiler_params=pltpu.CompilerParams(
            collective_id=0, has_side_effects=True, vmem_limit_bytes=52 * 1024 * 1024
        ),
        name="main",
    )(
        block_input, out_grad, w_value, w_gate, w_proj, conv_taps,
        norm_gain.reshape(1, chans), norm_shift.reshape(1, chans),
    )
    outs = pl.pallas_call(
        finish_kernel,
        out_shape=(
            shape((tokens, cols), BF), shape((rows, chans), F32), shape((rows, chans), F32),
            shape((chans, rows), F32), shape((kernel_len, chans), F32), shape((1, chans), F32), shape((1, chans), F32),
        ),
        in_specs=[vmem] * 4,
        out_specs=(anywhere,) * 7,
        scratch_shapes=[
            V((kernel_len, chans), F32), V((1, chans), F32), V((1, chans), F32), dma((5 + 2 * halves,)),
        ],
        compiler_params=pltpu.CompilerParams(vmem_limit_bytes=4 * 1024 * 1024),
        name="finish",
    )(*results)
    return outs[:5] + (outs[5].reshape(chans), outs[6].reshape(chans))


def solution(mesh):
    return jax.shard_map(
        shards,
        mesh=mesh,
        in_specs=(
            P("sp", None),
            P("sp", None),
            P(None, "tp"),
            P(None, "tp"),
            P(None, "tp"),
            P("tp"),
            P("tp"),
            P("tp", None),
        ),
        out_specs=(
            P("sp", "tp"),
            P("sp", "tp"),
            P("sp", "tp"),
            P("tp", "sp"),
            P(None, "tp"),
            P("tp"),
            P("tp"),
        ),
        check_vma=False,
    )
```

```python
import functools
import math

import jax
import jax.numpy as jnp
from jax import lax
from jax.experimental import pallas as pl
from jax.experimental.pallas import tpu as pltpu
from jax.sharding import PartitionSpec as P

EPS = 0.05
MESH = pl.DeviceIdType.MESH
LANES = 128
BF, F32 = jnp.bfloat16, jnp.float32


def right_product(left, right):
    return lax.dot_general(
        left, right, (((1,), (1,)), ((), ())), preferred_element_type=F32
    )


def column_product(left, right):
    return lax.dot_general(
        left, right, (((0,), (0,)), ((), ())), preferred_element_type=F32
    )


def main_kernel(
    n, n_tp, n_chan, halo,
    bi_hbm, og_hbm, wv_hbm, wg_hbm, wp_hbm, taps_hbm, gain_hbm, shift_hbm,
    ig_ref, ws_ref, ps_ref, sm_ref,
    bi, og, ww, wp, taps_ref, gain_ref, shift_ref,
    gx, vp, sg, fl, nm, gn, gf, gm, mo, gb, turned, tacc, cols, rowbuf, so, si,
    part, own, mate_in, low_out, low_in, far_out, far_in,
    xs, xr, ys, yr, acc, small, small_in, small_pair, small_all, small_sum,
    load_sem, st_send, st_recv, hx_send, hx_recv, hf_send, hf_recv,
    mate_send, mate_recv, low_send, low_recv, far_send, far_recv,
    x_send, x_recv, y_send, y_recv, s_send, s_recv, sa_send, sa_recv, sb_send, sb_recv,
):
    me, t = lax.axis_index("sp"), lax.axis_index("tp")
    outer, inner = me // 2, me % 2
    h = n // 2
    mate = 2 * outer + (1 - inner)
    t_near, t_far = t + 1 - 2 * (t % 2), lax.rem(t + n_tp // 2, n_tp)
    t_cross = lax.rem(t_near + n_tp // 2, n_tp)
    tokens, width = bi.shape
    rows, cols_tp = width // n, width // n_tp
    chans, halves = wp.shape[0], ww.shape[0]
    kernel_len = taps_ref.shape[0]
    chunks = xs.shape[0]
    step = tokens // chunks
    block = 64
    per = step // block

    def load(src, dst, i):
        copy = pltpu.make_async_copy(src, dst, load_sem.at[i])
        copy.start()
        return copy

    def piece(r):
        return pl.ds(r * step, step)

    order_in = [chunks - 1] + list(range(chunks - 1))
    load_w = []
    for c in range(halves):
        at = slice(c * LANES, (c + 1) * LANES)
        load_w.append(load(wv_hbm.at[:, at], ww.at[c, :, :LANES], 2 * c))
        load_w.append(load(wg_hbm.at[:, at], ww.at[c, :, LANES:], 2 * c + 1))
    def load_input(r):
        return load(bi_hbm.at[piece(r)], bi.at[piece(r)], 2 * halves + r)

    load_bi = {order_in[0]: load_input(order_in[0])}

    barrier = pltpu.get_barrier_semaphore()
    group = h // 4
    levels = group.bit_length() - 1
    place, low = outer // group, outer % group
    low_flips = [(1 << q) * (1 - 2 * ((low // (1 << q)) % 2)) for q in range(levels)]
    flip_near, flip_far = 1 - 2 * (place % 2), 2 - 4 * (place // 2)
    edge = 1 - (place % 2 + place // 2) % 2
    ends = [
        place + flip_near + edge * flip_far, place + flip_far,
        place + flip_near + (1 - edge) * flip_far, place,
    ]

    def outer_of(spot, mask):
        return spot * group + sum((low_flips[q] for q in range(levels) if mask >> q & 1), low)

    peers = [{"sp": 2 * lax.rem(outer + k, h) + inner} for k in range(1, h)]
    peers += [{"sp": mate}, {"sp": lax.rem(me + 1, n)}, {"sp": lax.rem(me + n - 1, n)}]
    peers += [{"tp": lax.rem(t + k, n_tp)} for k in range(1, n_tp)]
    for who in peers:
        pl.semaphore_signal(barrier, inc=1, device_id=who, device_id_type=MESH)

    first, last = me == 0, me == n - 1
    tacc[...] = jnp.zeros_like(tacc)

    @pl.when(first)
    def _():
        gx[:, :halo, :] = jnp.zeros((halves, halo, LANES), F32)

    @pl.when(last)
    def _():
        gf[:, tokens:, :] = jnp.zeros((halves, halo, LANES), F32)

    def describe(src, dst, send_sem, recv_sem, who):
        return pltpu.make_async_remote_copy(
            src_ref=src, dst_ref=dst, send_sem=send_sem, recv_sem=recv_sem,
            device_id=who, device_id_type=MESH,
        )

    def send(*args):
        copy = describe(*args)
        copy.start()
        return copy

    sent = []

    halo_x = describe(
        gx.at[:, pl.ds(tokens, halo), :], gx.at[:, pl.ds(0, halo), :],
        hx_send.at[0], hx_recv.at[0], {"sp": lax.rem(me + 1, n)},
    )
    for copy in load_w:
        copy.wait()
    for r in order_in[1:]:
        load_bi[r] = load_input(r)
    at_sem = 2 * halves + chunks
    load_small = [
        load(src, dst, at_sem + 2 + i)
        for i, (src, dst) in enumerate(((taps_hbm, taps_ref), (gain_hbm, gain_ref), (shift_hbm, shift_ref)))
    ]
    for r in order_in:
        load_bi[r].wait()
        if r == order_in[1]:
            load_og, load_wp = load(og_hbm, og, at_sem + 1), load(wp_hbm, wp, at_sem)
        where = piece(r)
        for c in range(halves):
            at = slice(c * LANES, (c + 1) * LANES)
            both = jnp.dot(bi[where, :], ww[c], preferred_element_type=F32).astype(BF)
            value = both[:, :LANES]
            sigmoid = jax.nn.sigmoid(both[:, LANES:].astype(F32))
            vp[where, at] = value
            sg[where, at] = sigmoid
            gx[c, pl.ds(halo + r * step, step), :] = (value.astype(F32) * sigmoid).astype(BF).astype(F32)

    pl.semaphore_wait(barrier, len(peers))

    @pl.when(me < n - 1)
    def _():
        halo_x.start()

    for copy in load_small:
        copy.wait()

    lane = lax.broadcasted_iota(jnp.int32, (block, LANES), 1)

    def send_stats(phase, r):
        so[phase, r] = rowbuf[...].T[:8]
        copies = [
            send(so.at[phase, r], si.at[phase, r, k - 1], st_send.at[phase, r, k - 1],
                 st_recv.at[phase, r, k - 1], {"tp": lax.rem(t + k, n_tp)})
            for k in range(1, n_tp)
        ]
        sent.extend(copies)
        return copies

    def take_stats(phase, r, copies):
        total = so[phase, r]
        for k, copy in enumerate(copies):
            copy.wait_recv()
            total = total + si[phase, r, k]
        return total / n_chan

    def rows_of(base, i):
        return pl.ds(pl.multiple_of(base + i * block, block), block)

    def pair_of_sums(i, first_sum, second_sum):
        rowbuf[rows_of(0, i), :] = jnp.where(
            lane == 0, first_sum, jnp.where(lane == 1, second_sum, 0.0)
        )

    def conv_chunk(r):
        def body(i, carry):
            sums = jnp.zeros((block, LANES), F32)
            squares = jnp.zeros((block, LANES), F32)
            for c in range(halves):
                total = jnp.zeros((block, LANES), F32)
                for k in range(kernel_len):
                    where = pl.ds(r * step + i * block + halo - k, block)
                    total = total + taps_ref[pl.ds(k, 1), c * LANES:(c + 1) * LANES] * gx[c, where, :]
                fl[c, rows_of(r * step, i), :] = total
                sums = sums + total
                squares = squares + total * total
            pair_of_sums(i, jnp.sum(sums, axis=1, keepdims=True), jnp.sum(squares, axis=1, keepdims=True))
            return carry

        lax.fori_loop(0, per, body, 0, unroll=True)
        return send_stats(0, r)

    late_first = list(range(1, chunks)) + [0]
    moments, means = {}, {}
    for r in late_first:
        if r == 0:
            @pl.when(me > 0)
            def _():
                halo_x.wait_recv()
        moments[r] = conv_chunk(r)

    def norm_chunk(r):
        total = take_stats(0, r, moments[r])
        mean = total[0:1]
        scale = lax.rsqrt(total[1:2] - mean * mean + EPS)
        both = jnp.where(lax.broadcasted_iota(jnp.int32, total.shape, 0) == 0, mean, scale)
        cols[0, piece(r), :8] = both.T

        def body(i, carry):
            where = rows_of(r * step, i)
            mean = cols[0, where, 0:1]
            scale = cols[0, where, 1:2]
            for c in range(halves):
                at = slice(c * LANES, (c + 1) * LANES)
                normed = (fl[c, where, :] - mean) * scale
                activated = normed * gain_ref[:, at] + shift_ref[:, at]
                sigmoid = jax.nn.sigmoid(activated)
                mo[where, at] = (activated * sigmoid).astype(BF)
                nm[c, where, :] = normed
                fl[c, where, :] = sigmoid
            return carry

        lax.fori_loop(0, per, body, 0, unroll=True)

    def cotangent_chunk(r, carry):
        def body(i, carry):
            where = rows_of(r * step, i)
            sums = jnp.zeros((block, LANES), F32)
            crosses = jnp.zeros((block, LANES), F32)
            out = []
            for c in range(halves):
                at = slice(c * LANES, (c + 1) * LANES)
                gain = gain_ref[:, at]
                normed = nm[c, where, :]
                activated = normed * gain + shift_ref[:, at]
                sigmoid = fl[c, where, :]
                grad_act = gm[where, at] * sigmoid * (1.0 + activated * (1.0 - sigmoid))
                grad_normed = grad_act * gain
                gn[c, where, :] = grad_normed
                sums = sums + grad_normed
                crosses = crosses + grad_normed * normed
                fold = lambda x: x.reshape(block // 8, 8, LANES).sum(axis=0)
                out.append(carry[2 * c] + fold(grad_act * normed))
                out.append(carry[2 * c + 1] + fold(grad_act))
            pair_of_sums(i, jnp.sum(sums, axis=1, keepdims=True), jnp.sum(crosses, axis=1, keepdims=True))
            return tuple(out)

        carry = lax.fori_loop(0, per, body, carry, unroll=True)
        return send_stats(1, r), carry

    def mix(r):
        mixed = [right_product(og[piece(i), :], wp[...]) for i in (r, r + 1)]
        gm[piece(r), :] = mixed[0]
        gm[piece(r + 1), :] = mixed[1]

    load_wp.wait()
    load_og.wait()
    mix(0)
    for r in late_first:
        norm_chunk(r)

    aligned = rows % LANES == 0
    wide = 256

    blocks_of = [(mask, i) for mask in range(group - 1, -1, -1) for i in range(4)]
    acts = [og] + [bi] * halves
    mate_copies = [[] for _ in acts]
    low_copies = [{} for _ in acts]
    far_copies = [[] for _ in acts]

    def device_block(k, i):
        mask, spot = blocks_of[k]
        return 2 * outer_of(ends[spot], mask) + i

    def make_others(j, other):
        if aligned:
            turned[j] = other.T
        else:
            for w in range(width // wide):
                found = column_product(acts[j][:, w * wide:(w + 1) * wide], other).astype(BF)
                part[j, pl.ds(w * (wide // rows), wide // rows)] = found.reshape(wide // rows, rows, found.shape[1])

    def product(j, b):
        where = pl.ds(pl.multiple_of(b * rows, rows), rows)
        return jnp.dot(turned[j], acts[j][:, where], preferred_element_type=F32)

    def make_mates(j, ks):
        blocks = [device_block(k, 1 - inner) for k in ks]
        if aligned:
            found = [product(j, b) for b in blocks]
            for b, block in zip(blocks, found):
                part[j, b] = block.astype(BF)

    def send_mates(j, ks):
        for k in ks:
            b = device_block(k, 1 - inner)
            mate_copies[j].append(send(
                part.at[j, b], mate_in.at[j, k], mate_send.at[j, k], mate_recv.at[j, k], {"sp": mate}
            ))

    pairs = [range(k, min(k + 2, h)) for k in range(0, h, 2)]

    def mate_blocks(j):
        for ks in pairs:
            make_mates(j, ks)
            send_mates(j, [k for k in ks if k < h - 1])

    def landed(j, slot):
        return describe(
            far_out.at[j, 0], far_in.at[j, slot], far_send.at[j, 0], far_recv.at[j, slot], {"sp": mate}
        )

    def far_step(j, k):
        mask, i = blocks_of[k]
        b = device_block(k, inner)
        total = product(j, b) if aligned else part[j, b].astype(F32)
        mate_copies[j][k].wait_recv()
        total = total + mate_in[j, k].astype(F32)
        lowest = [q for q in range(levels) if mask >> q & 1][:1] or [levels]
        for q in range(lowest[0]):
            came = mask + (1 << q)
            low_copies[j][came, i].wait_recv()
            total = total + low_in[j, (came - 1) * 4 + i].astype(F32)
        if mask:
            at = (mask - 1) * 4 + i
            low_out[j, at] = total.astype(BF)
            low_copies[j][mask, i] = send(
                low_out.at[j, at], low_in.at[j, at], low_send.at[j, at], low_recv.at[j, at],
                {"sp": 2 * outer_of(place, 1 << lowest[0]) + inner},
            )
            return
        if i == 3:
            own[j] = total
            return
        if i:
            @pl.when(edge == 0)
            def _():
                landed(j, i - 1).wait_recv()
                far_out[j, i] = (total + far_in[j, i - 1].astype(F32)).astype(BF)

            @pl.when(edge == 1)
            def _():
                far_out[j, i] = total.astype(BF)

            slot = edge * i + (1 - edge) * 3
            target = edge * (place + flip_near) + (1 - edge) * ends[i]
        else:
            far_out[j, i] = total.astype(BF)
            slot, target = (1 - edge) * 2, place + flip_near
        far_copies[j].append(send(
            far_out.at[j, i], far_in.at[j, slot], far_send.at[j, i], far_recv.at[j, slot],
            {"sp": 2 * outer_of(target, 0) + inner},
        ))

    def whole(j):
        total = own[j]
        for slot in (2, 3):
            landed(j, slot).wait_recv()
            total = total + far_in[j, slot].astype(F32)
        return total * loss_scale

    make_others(0, mo[...])
    make_mates(0, pairs[0])
    send_mates(0, pairs[0])

    carry = tuple(jnp.zeros((8, LANES), F32) for _ in range(2 * halves))
    for r in range(0, chunks, 2):
        if r:
            mix(r)
        for i in (r, r + 1):
            means[i], carry = cotangent_chunk(i, carry)
    for ks in pairs[1:]:
        make_mates(0, ks)
    small[...] = jnp.zeros_like(small)
    for c in range(halves):
        small[c, kernel_len:kernel_len + 1] = carry[2 * c].sum(axis=0, keepdims=True)
        small[c, kernel_len + 1:kernel_len + 2] = carry[2 * c + 1].sum(axis=0, keepdims=True)

    halo_f = describe(
        gf.at[:, pl.ds(0, halo), :], gf.at[:, pl.ds(tokens, halo), :],
        hf_send.at[0], hf_recv.at[0], {"sp": lax.rem(me + n - 1, n)},
    )

    def filtered_chunk(r):
        cols[1, piece(r), :8] = take_stats(1, r, means[r]).T

        def body(i, carry):
            where = rows_of(r * step, i)
            scale = cols[0, where, 1:2]
            first_mean = cols[1, where, 0:1]
            second_mean = cols[1, where, 1:2]
            for c in range(halves):
                gf[c, where, :] = scale * (
                    gn[c, where, :] - first_mean - nm[c, where, :] * second_mean
                )
            return carry

        lax.fori_loop(0, per, body, 0, unroll=True)

    def back_chunk(r, c):
        at = slice(c * LANES, (c + 1) * LANES)

        def body(i, carry):
            where = rows_of(r * step, i)
            gated = gx[c, pl.ds(pl.multiple_of(r * step + i * block + halo, 8), block), :]
            total = jnp.zeros((block, LANES), F32)
            for k in range(kernel_len):
                grad = gf[c, pl.ds(r * step + i * block + k, block), :]
                total = total + taps_ref[pl.ds(k, 1), at] * grad
                tacc[c, k] += (gated * grad).reshape(block // 8, 8, LANES).sum(axis=0)
            sigmoid = sg[where, at]
            value = vp[where, at].astype(F32)
            gb[c, where, :LANES] = (total * sigmoid).astype(BF)
            gb[c, where, LANES:] = (total * value * sigmoid * (1.0 - sigmoid)).astype(BF)
            return carry

        lax.fori_loop(0, per, body, 0)

    def partial_input(r, j):
        at = pl.ds(pl.multiple_of(j * cols_tp, cols_tp), cols_tp)
        total = right_product(gb[0, piece(r), :], ww[0, at, :])
        for c in range(1, halves):
            total = total + right_product(gb[c, piece(r), :], ww[c, at, :])
        return total

    x_copies, y_copies = [], []

    def near_block(r):
        xs[r, 0] = partial_input(r, t_cross).astype(BF)
        xs[r, 1] = partial_input(r, t_near).astype(BF)
        x_copies.append(send(xs.at[r], xr.at[r], x_send.at[r], x_recv.at[r], {"tp": t_near}))

    def far_block(r):
        far = partial_input(r, t_far)
        acc[piece(r), :] = partial_input(r, t)
        x_copies[r].wait_recv()
        ys[r] = (far + xr[r, 0].astype(F32)).astype(BF)
        y_copies.append(send(ys.at[r], yr.at[r], y_send.at[r], y_recv.at[r], {"tp": t_far}))
        acc[piece(r), :] += xr[r, 1].astype(F32)

    filtered_chunk(0)

    @pl.when(me > 0)
    def _():
        halo_f.start()

    for ks in pairs[1:]:
        send_mates(0, ks)
    todo = [(j, k) for j in range(1 + halves) for k in range(h - 1)]
    for r in range(1, chunks):
        filtered_chunk(r)


    def far_steps(count):
        for _ in range(count):
            far_step(*todo.pop(0))

    for c in range(halves):
        back_chunk(0, c)
    far_steps(1)
    near_block(0)
    for c in range(halves):
        for r in range(1, chunks):
            if c == 0 and r == chunks - 1:
                @pl.when(me < n - 1)
                def _():
                    halo_f.wait_recv()
            back_chunk(r, c)
            if c == 0 and r == 1:
                far_block(0)
            if c == halves - 1:
                near_block(r)
                if r > 1:
                    far_block(r - 1)
                    far_steps(1)
        small[c, :kernel_len] = tacc[c].sum(axis=1)
        if c == halves - 1:
            small_copy = send(small.at[1 - inner], small_in, s_send.at[0], s_recv.at[0], {"sp": mate})
        make_others(1 + c, gb[c])
        mate_blocks(1 + c)
        if c == 0:
            far_steps(1)
    for c in range(halves):
        send_mates(1 + c, [h - 1])
    far_block(chunks - 1)

    loss_scale = 1.0 / math.sqrt(tokens * n)
    def input_chunk(r):
        y_copies[r].wait_recv()
        ig_ref[piece(r), :] = (acc[piece(r), :] + yr[r].astype(F32)).astype(BF)

    def weight_half(c):
        total = whole(1 + c)
        ws_ref[c] = total.T if aligned else total

    far_steps(len(todo) - (h - 1))
    small_copy.wait_recv()
    small_pair[...] = small[inner] + small_in[...]
    small_copies = [
        send(small_pair, small_all.at[outer], sa_send.at[k - 1], sa_recv.at[k - 1],
             {"sp": 2 * lax.rem(outer + k, h) + inner})
        for k in range(1, h)
    ]
    far_step(0, h - 1)
    total = whole(0)
    ps_ref[...] = total if aligned else total.T
    far_steps(len(todo) - 1)
    for copy in small_copies:
        copy.wait_recv()
    small_all[outer] = small_pair[...]
    total = small_all[0]
    for k in range(1, h):
        total = total + small_all[k]
    small_sum[inner] = total * loss_scale
    half_copy = send(
        small_sum.at[inner], small_sum.at[inner], sb_send.at[0], sb_recv.at[0], {"sp": mate}
    )
    for r in range(chunks - 1):
        input_chunk(r)
    far_steps(1)
    input_chunk(chunks - 1)
    for c in range(halves):
        far_step(1 + c, h - 1)
        weight_half(c)
    half_copy.wait_recv()
    sm_ref[...] = small_sum[...]

    @pl.when(me < n - 1)
    def _():
        halo_x.wait_send()

    @pl.when(me > 0)
    def _():
        halo_f.wait_send()

    for copies in mate_copies + far_copies + [list(found.values()) for found in low_copies]:
        sent.extend(copies)
    for copy in sent + x_copies + y_copies + small_copies + [small_copy, half_copy]:
        copy.wait_send()


def finish_kernel(
    ig_ref, ws_ref, ps_ref, sm_ref, ig_out, wv_out, wg_out, wp_out, taps_out, gain_out, shift_out,
    taps, gain, shift, sems,
):
    chans = ps_ref.shape[0]
    kernel_len = taps_out.shape[0]
    copies = []

    def store(src, dst):
        copies.append(pltpu.make_async_copy(src, dst, sems.at[len(copies)]))
        copies[-1].start()

    store(ig_ref, ig_out)
    store(ps_ref, wp_out)
    for c in range(chans // LANES):
        at = slice(c * LANES, (c + 1) * LANES)
        store(ws_ref.at[c, :, :LANES], wv_out.at[:, at])
        store(ws_ref.at[c, :, LANES:], wg_out.at[:, at])
        taps[:, at] = sm_ref[c, :kernel_len]
        gain[:, at] = sm_ref[c, kernel_len:kernel_len + 1]
        shift[:, at] = sm_ref[c, kernel_len + 1:kernel_len + 2]
    store(taps, taps_out)
    store(gain, gain_out)
    store(shift, shift_out)
    for copy in copies:
        copy.wait()


def shards(block_input, out_grad, w_value, w_gate, conv_taps, norm_gain, norm_shift, w_proj):
    n, n_tp = lax.axis_size("sp"), lax.axis_size("tp")
    tokens, width = block_input.shape
    chans = w_value.shape[1]
    kernel_len = conv_taps.shape[0]
    halves = chans // LANES
    halo = -(-(kernel_len - 1) // 8) * 8
    rows, cols, h, chunks = width // n, width // n_tp, n // 2, 4
    step = tokens // chunks
    smalls = (-(-(kernel_len + 2) // 8) * 8, LANES)
    pair, sums, lows = 2 * LANES, 1 + halves, max(h - 4, 1)
    part = (pair, rows) if rows % LANES == 0 else (rows, pair)
    anywhere = pl.BlockSpec(memory_space=pl.ANY)
    vmem = pl.BlockSpec(memory_space=pltpu.VMEM)
    dma = pltpu.SemaphoreType.DMA
    V = pltpu.VMEM
    shape = jax.ShapeDtypeStruct
    results = pl.pallas_call(
        functools.partial(main_kernel, n, n_tp, chans * n_tp, halo),
        out_shape=(
            shape((tokens, cols), BF), shape((halves, rows, pair), F32),
            shape((chans, rows), F32), shape((halves,) + smalls, F32),
        ),
        in_specs=[pl.BlockSpec(memory_space=pltpu.HBM)] * 8,
        out_specs=(vmem,) * 4,
        scratch_shapes=[
            V((tokens, width), BF), V((tokens, width), BF), V((halves, width, pair), BF),
            V((chans, width), BF), V((kernel_len, chans), F32), V((1, chans), F32), V((1, chans), F32),
            V((halves, halo + tokens, LANES), F32), V((tokens, chans), BF), V((tokens, chans), F32),
            V((halves, tokens, LANES), F32), V((halves, tokens, LANES), F32), V((halves, tokens, LANES), F32),
            V((halves, tokens + halo, LANES), F32), V((tokens, chans), F32), V((tokens, chans), BF),
            V((halves, tokens, pair), BF), V((sums, pair, tokens), BF), V((halves, kernel_len, 8, LANES), F32), V((2, tokens, LANES), F32),
            V((step, LANES), F32), V((2, chunks, 8, step), F32), V((2, chunks, n_tp - 1, 8, step), F32),
            V((sums, n) + part, BF), V((sums,) + part, F32), V((sums, h) + part, BF), V((sums, lows) + part, BF), V((sums, lows) + part, BF),
            V((sums, 3) + part, BF), V((sums, 4) + part, BF),
            V((chunks, 2, step, cols), BF), V((chunks, 2, step, cols), BF), V((chunks, step, cols), BF),
            V((chunks, step, cols), BF), V((tokens, cols), F32),
            V((halves,) + smalls, F32), V(smalls, F32), V(smalls, F32), V((h,) + smalls, F32),
            V((halves,) + smalls, F32),
            dma((2 * halves + chunks + 5,)), dma((2, chunks, n_tp - 1)), dma((2, chunks, n_tp - 1)),
            dma((1,)), dma((1,)), dma((1,)), dma((1,)),
            dma((sums, h)), dma((sums, h)), dma((sums, lows)), dma((sums, lows)), dma((sums, 3)), dma((sums, 4)),
            dma((chunks,)), dma((chunks,)), dma((chunks,)), dma((chunks,)), dma((1,)), dma((1,)),
            dma((h - 1,)), dma((h - 1,)), dma((1,)), dma((1,)),
        ],
        compiler_params=pltpu.CompilerParams(
            collective_id=0, has_side_effects=True, vmem_limit_bytes=52 * 1024 * 1024
        ),
        name="main",
    )(*[
        pltpu.with_memory_space_constraint(x, pltpu.HBM)
        for x in (
            block_input, out_grad, w_value, w_gate, w_proj, conv_taps,
            norm_gain.reshape(1, chans), norm_shift.reshape(1, chans),
        )
    ])
    outs = pl.pallas_call(
        finish_kernel,
        out_shape=(
            shape((tokens, cols), BF), shape((rows, chans), F32), shape((rows, chans), F32),
            shape((chans, rows), F32), shape((kernel_len, chans), F32), shape((1, chans), F32), shape((1, chans), F32),
        ),
        in_specs=[vmem] * 4,
        out_specs=(anywhere,) * 7,
        scratch_shapes=[
            V((kernel_len, chans), F32), V((1, chans), F32), V((1, chans), F32), dma((5 + 2 * halves,)),
        ],
        compiler_params=pltpu.CompilerParams(vmem_limit_bytes=4 * 1024 * 1024),
        name="finish",
    )(*results)
    return outs[:5] + (outs[5].reshape(chans), outs[6].reshape(chans))


def solution(mesh):
    return jax.shard_map(
        shards,
        mesh=mesh,
        in_specs=(
            P("sp", None),
            P("sp", None),
            P(None, "tp"),
            P(None, "tp"),
            P(None, "tp"),
            P("tp"),
            P("tp"),
            P("tp", None),
        ),
        out_specs=(
            P("sp", "tp"),
            P("sp", "tp"),
            P("sp", "tp"),
            P("tp", "sp"),
            P(None, "tp"),
            P("tp"),
            P("tp"),
        ),
        check_vma=False,
    )
```

```python
import functools
import math

import jax
import jax.numpy as jnp
from jax import lax
from jax.experimental import pallas as pl
from jax.experimental.pallas import tpu as pltpu
from jax.sharding import PartitionSpec as P

EPS = 0.05
MESH = pl.DeviceIdType.MESH
LANES = 128
BF, F32 = jnp.bfloat16, jnp.float32


def right_product(left, right):
    return lax.dot_general(
        left, right, (((1,), (1,)), ((), ())), preferred_element_type=F32
    )


def column_product(left, right):
    return lax.dot_general(
        left, right, (((0,), (0,)), ((), ())), preferred_element_type=F32
    )


def main_kernel(
    n, n_tp, n_chan, halo,
    bi_hbm, og_hbm, wv_hbm, wg_hbm, wp_hbm, taps_hbm, gain_hbm, shift_hbm,
    ig_ref, ws_ref, ps_ref, sm_ref,
    bi, og, ww, wp, taps_ref, gain_ref, shift_ref,
    gx, vp, sg, fl, nm, gn, gf, gm, mo, gb, turned, tacc, cols, rowbuf, so, si,
    part, own, mate_in, low_out, low_in, far_out, far_in,
    xs, xr, ys, yr, acc, small, small_in, small_pair, small_all, small_sum,
    load_sem, st_send, st_recv, hx_send, hx_recv, hf_send, hf_recv,
    mate_send, mate_recv, low_send, low_recv, far_send, far_recv,
    x_send, x_recv, y_send, y_recv, s_send, s_recv, sa_send, sa_recv, sb_send, sb_recv,
):
    me, t = lax.axis_index("sp"), lax.axis_index("tp")
    outer, inner = me // 2, me % 2
    h = n // 2
    mate = 2 * outer + (1 - inner)
    t_near, t_far = t + 1 - 2 * (t % 2), lax.rem(t + n_tp // 2, n_tp)
    t_cross = lax.rem(t_near + n_tp // 2, n_tp)
    tokens, width = bi.shape
    rows, cols_tp = width // n, width // n_tp
    chans, halves = wp.shape[0], ww.shape[0]
    kernel_len = taps_ref.shape[0]
    chunks = xs.shape[0]
    step = tokens // chunks
    block = 64
    per = step // block

    def load(src, dst, i):
        copy = pltpu.make_async_copy(src, dst, load_sem.at[i])
        copy.start()
        return copy

    def piece(r):
        return pl.ds(r * step, step)

    order_in = [chunks - 1] + list(range(chunks - 1))
    load_w = []
    for c in range(halves):
        at = slice(c * LANES, (c + 1) * LANES)
        load_w.append(load(wv_hbm.at[:, at], ww.at[c, :, :LANES], 2 * c))
        load_w.append(load(wg_hbm.at[:, at], ww.at[c, :, LANES:], 2 * c + 1))
    def load_input(r):
        return load(bi_hbm.at[piece(r)], bi.at[piece(r)], 2 * halves + r)

    load_bi = {order_in[0]: load_input(order_in[0])}

    barrier = pltpu.get_barrier_semaphore()
    group = h // 4
    levels = group.bit_length() - 1
    place, low = outer // group, outer % group
    low_flips = [(1 << q) * (1 - 2 * ((low // (1 << q)) % 2)) for q in range(levels)]
    flip_near, flip_far = 1 - 2 * (place % 2), 2 - 4 * (place // 2)
    edge = 1 - (place % 2 + place // 2) % 2
    ends = [
        place + flip_near + edge * flip_far, place + flip_far,
        place + flip_near + (1 - edge) * flip_far, place,
    ]

    def outer_of(spot, mask):
        return spot * group + sum((low_flips[q] for q in range(levels) if mask >> q & 1), low)

    peers = [{"sp": 2 * lax.rem(outer + k, h) + inner} for k in range(1, h)]
    peers += [{"sp": mate}, {"sp": lax.rem(me + 1, n)}, {"sp": lax.rem(me + n - 1, n)}]
    peers += [{"tp": lax.rem(t + k, n_tp)} for k in range(1, n_tp)]
    for who in peers:
        pl.semaphore_signal(barrier, inc=1, device_id=who, device_id_type=MESH)

    first, last = me == 0, me == n - 1
    tacc[...] = jnp.zeros_like(tacc)

    @pl.when(first)
    def _():
        gx[:, :halo, :] = jnp.zeros((halves, halo, LANES), F32)

    @pl.when(last)
    def _():
        gf[:, tokens:, :] = jnp.zeros((halves, halo, LANES), F32)

    def describe(src, dst, send_sem, recv_sem, who):
        return pltpu.make_async_remote_copy(
            src_ref=src, dst_ref=dst, send_sem=send_sem, recv_sem=recv_sem,
            device_id=who, device_id_type=MESH,
        )

    def send(*args):
        copy = describe(*args)
        copy.start()
        return copy

    sent = []

    halo_x = describe(
        gx.at[:, pl.ds(tokens, halo), :], gx.at[:, pl.ds(0, halo), :],
        hx_send.at[0], hx_recv.at[0], {"sp": lax.rem(me + 1, n)},
    )
    for copy in load_w:
        copy.wait()
    for r in order_in[1:]:
        load_bi[r] = load_input(r)
    at_sem = 2 * halves + chunks
    load_small = [
        load(src, dst, at_sem + 2 + i)
        for i, (src, dst) in enumerate(((taps_hbm, taps_ref), (gain_hbm, gain_ref), (shift_hbm, shift_ref)))
    ]
    for r in order_in:
        load_bi[r].wait()
        if r == order_in[1]:
            load_og, load_wp = load(og_hbm, og, at_sem + 1), load(wp_hbm, wp, at_sem)
        where = piece(r)
        for c in range(halves):
            at = slice(c * LANES, (c + 1) * LANES)
            both = jnp.dot(bi[where, :], ww[c], preferred_element_type=F32).astype(BF)
            value = both[:, :LANES]
            sigmoid = jax.nn.sigmoid(both[:, LANES:].astype(F32))
            vp[where, at] = value
            sg[where, at] = sigmoid
            gx[c, pl.ds(halo + r * step, step), :] = (value.astype(F32) * sigmoid).astype(BF).astype(F32)
        if r == order_in[0]:
            pl.semaphore_wait(barrier, len(peers))

            @pl.when(me < n - 1)
            def _():
                halo_x.start()


    for copy in load_small:
        copy.wait()

    lane = lax.broadcasted_iota(jnp.int32, (block, LANES), 1)

    def send_stats(phase, r):
        so[phase, r] = rowbuf[...].T[:8]
        copies = [
            send(so.at[phase, r], si.at[phase, r, k - 1], st_send.at[phase, r, k - 1],
                 st_recv.at[phase, r, k - 1], {"tp": lax.rem(t + k, n_tp)})
            for k in range(1, n_tp)
        ]
        sent.extend(copies)
        return copies

    def take_stats(phase, r, copies):
        total = so[phase, r]
        for k, copy in enumerate(copies):
            copy.wait_recv()
            total = total + si[phase, r, k]
        return total / n_chan

    def rows_of(base, i):
        return pl.ds(pl.multiple_of(base + i * block, block), block)

    def pair_of_sums(i, first_sum, second_sum):
        rowbuf[rows_of(0, i), :] = jnp.where(
            lane == 0, first_sum, jnp.where(lane == 1, second_sum, 0.0)
        )

    def conv_chunk(r):
        def body(i, carry):
            sums = jnp.zeros((block, LANES), F32)
            squares = jnp.zeros((block, LANES), F32)
            for c in range(halves):
                total = jnp.zeros((block, LANES), F32)
                for k in range(kernel_len):
                    where = pl.ds(r * step + i * block + halo - k, block)
                    total = total + taps_ref[pl.ds(k, 1), c * LANES:(c + 1) * LANES] * gx[c, where, :]
                fl[c, rows_of(r * step, i), :] = total
                sums = sums + total
                squares = squares + total * total
            pair_of_sums(i, jnp.sum(sums, axis=1, keepdims=True), jnp.sum(squares, axis=1, keepdims=True))
            return carry

        lax.fori_loop(0, per, body, 0, unroll=True)
        return send_stats(0, r)

    order_conv = [1, 0] + list(range(2, chunks))
    moments, means = {}, {}
    for r in order_conv:
        if r == 0:
            @pl.when(me > 0)
            def _():
                halo_x.wait_recv()
        moments[r] = conv_chunk(r)

    def norm_chunk(r):
        total = take_stats(0, r, moments[r])
        mean = total[0:1]
        scale = lax.rsqrt(total[1:2] - mean * mean + EPS)
        both = jnp.where(lax.broadcasted_iota(jnp.int32, total.shape, 0) == 0, mean, scale)
        cols[0, piece(r), :8] = both.T

        def body(i, carry):
            where = rows_of(r * step, i)
            mean = cols[0, where, 0:1]
            scale = cols[0, where, 1:2]
            for c in range(halves):
                at = slice(c * LANES, (c + 1) * LANES)
                normed = (fl[c, where, :] - mean) * scale
                activated = normed * gain_ref[:, at] + shift_ref[:, at]
                sigmoid = jax.nn.sigmoid(activated)
                mo[where, at] = (activated * sigmoid).astype(BF)
                nm[c, where, :] = normed
                fl[c, where, :] = sigmoid
            return carry

        lax.fori_loop(0, per, body, 0, unroll=True)

    def cotangent_chunk(r, carry):
        def body(i, carry):
            where = rows_of(r * step, i)
            sums = jnp.zeros((block, LANES), F32)
            crosses = jnp.zeros((block, LANES), F32)
            out = []
            for c in range(halves):
                at = slice(c * LANES, (c + 1) * LANES)
                gain = gain_ref[:, at]
                normed = nm[c, where, :]
                activated = normed * gain + shift_ref[:, at]
                sigmoid = fl[c, where, :]
                grad_act = gm[where, at] * sigmoid * (1.0 + activated * (1.0 - sigmoid))
                grad_normed = grad_act * gain
                gn[c, where, :] = grad_normed
                sums = sums + grad_normed
                crosses = crosses + grad_normed * normed
                fold = lambda x: x.reshape(block // 8, 8, LANES).sum(axis=0)
                out.append(carry[2 * c] + fold(grad_act * normed))
                out.append(carry[2 * c + 1] + fold(grad_act))
            pair_of_sums(i, jnp.sum(sums, axis=1, keepdims=True), jnp.sum(crosses, axis=1, keepdims=True))
            return tuple(out)

        carry = lax.fori_loop(0, per, body, carry, unroll=True)
        return send_stats(1, r), carry

    def mix(r):
        mixed = [right_product(og[piece(i), :], wp[...]) for i in (r, r + 1)]
        gm[piece(r), :] = mixed[0]
        gm[piece(r + 1), :] = mixed[1]

    load_wp.wait()
    load_og.wait()
    mix(0)
    carry = tuple(jnp.zeros((8, LANES), F32) for _ in range(2 * halves))
    for r in order_conv[:-1]:
        norm_chunk(r)
    for r in range(2):
        means[r], carry = cotangent_chunk(r, carry)
    norm_chunk(order_conv[-1])

    aligned = rows % LANES == 0
    wide = 256

    blocks_of = [(mask, i) for mask in range(group - 1, -1, -1) for i in range(4)]
    acts = [og] + [bi] * halves
    mate_copies = [[] for _ in acts]
    low_copies = [{} for _ in acts]
    far_copies = [[] for _ in acts]

    def device_block(k, i):
        mask, spot = blocks_of[k]
        return 2 * outer_of(ends[spot], mask) + i

    def make_others(j, other):
        if aligned:
            turned[j] = other.T
        else:
            for w in range(width // wide):
                found = column_product(acts[j][:, w * wide:(w + 1) * wide], other).astype(BF)
                part[j, pl.ds(w * (wide // rows), wide // rows)] = found.reshape(wide // rows, rows, found.shape[1])

    def product(j, b):
        where = pl.ds(pl.multiple_of(b * rows, rows), rows)
        return jnp.dot(turned[j], acts[j][:, where], preferred_element_type=F32)

    def make_mates(j, ks):
        blocks = [device_block(k, 1 - inner) for k in ks]
        if aligned:
            found = [product(j, b) for b in blocks]
            for b, block in zip(blocks, found):
                part[j, b] = block.astype(BF)

    def send_mates(j, ks):
        for k in ks:
            b = device_block(k, 1 - inner)
            mate_copies[j].append(send(
                part.at[j, b], mate_in.at[j, k], mate_send.at[j, k], mate_recv.at[j, k], {"sp": mate}
            ))

    pairs = [range(k, min(k + 2, h)) for k in range(0, h, 2)]

    def mate_blocks(j):
        for ks in pairs:
            make_mates(j, ks)
            send_mates(j, [k for k in ks if k < h - 1])

    def landed(j, slot):
        return describe(
            far_out.at[j, 0], far_in.at[j, slot], far_send.at[j, 0], far_recv.at[j, slot], {"sp": mate}
        )

    def far_step(j, k, only=None):
        mask, i = blocks_of[k]
        if not mask and i < 3 and only != 1:
            far_copies[j].append(describe(
                far_out.at[j, i], far_in.at[j, i], far_send.at[j, i], far_recv.at[j, i], {"sp": mate}
            ))
        if only is None:
            far_part(j, k)
        else:
            pl.when(edge == only)(lambda: far_part(j, k))

    def far_part(j, k):
        mask, i = blocks_of[k]
        b = device_block(k, inner)
        total = product(j, b) if aligned else part[j, b].astype(F32)
        mate_copies[j][k].wait_recv()
        total = total + mate_in[j, k].astype(F32)
        lowest = [q for q in range(levels) if mask >> q & 1][:1] or [levels]
        for q in range(lowest[0]):
            came = mask + (1 << q)
            low_copies[j][came, i].wait_recv()
            total = total + low_in[j, (came - 1) * 4 + i].astype(F32)
        if mask:
            at = (mask - 1) * 4 + i
            low_out[j, at] = total.astype(BF)
            low_copies[j][mask, i] = send(
                low_out.at[j, at], low_in.at[j, at], low_send.at[j, at], low_recv.at[j, at],
                {"sp": 2 * outer_of(place, 1 << lowest[0]) + inner},
            )
            return
        if i == 3:
            own[j] = total
            return
        if i:
            @pl.when(edge == 0)
            def _():
                landed(j, i - 1).wait_recv()
                far_out[j, i] = (total + far_in[j, i - 1].astype(F32)).astype(BF)

            @pl.when(edge == 1)
            def _():
                far_out[j, i] = total.astype(BF)

            slot = edge * i + (1 - edge) * 3
            target = edge * (place + flip_near) + (1 - edge) * ends[i]
        else:
            far_out[j, i] = total.astype(BF)
            slot, target = (1 - edge) * 2, place + flip_near
        send(
            far_out.at[j, i], far_in.at[j, slot], far_send.at[j, i], far_recv.at[j, slot],
            {"sp": 2 * outer_of(target, 0) + inner},
        )

    def whole(j):
        total = own[j]
        for slot in (2, 3):
            landed(j, slot).wait_recv()
            total = total + far_in[j, slot].astype(F32)
        return total * loss_scale

    make_others(0, mo[...])
    make_mates(0, pairs[0])
    send_mates(0, pairs[0])

    for r in range(2, chunks, 2):
        mix(r)
        for i in (r, r + 1):
            means[i], carry = cotangent_chunk(i, carry)
    for ks in pairs[1:]:
        make_mates(0, ks)
    small[...] = jnp.zeros_like(small)
    for c in range(halves):
        small[c, kernel_len:kernel_len + 1] = carry[2 * c].sum(axis=0, keepdims=True)
        small[c, kernel_len + 1:kernel_len + 2] = carry[2 * c + 1].sum(axis=0, keepdims=True)

    halo_f = describe(
        gf.at[:, pl.ds(0, halo), :], gf.at[:, pl.ds(tokens, halo), :],
        hf_send.at[0], hf_recv.at[0], {"sp": lax.rem(me + n - 1, n)},
    )

    def filtered_chunk(r):
        cols[1, piece(r), :8] = take_stats(1, r, means[r]).T

        def body(i, carry):
            where = rows_of(r * step, i)
            scale = cols[0, where, 1:2]
            first_mean = cols[1, where, 0:1]
            second_mean = cols[1, where, 1:2]
            for c in range(halves):
                gf[c, where, :] = scale * (
                    gn[c, where, :] - first_mean - nm[c, where, :] * second_mean
                )
            return carry

        lax.fori_loop(0, per, body, 0, unroll=True)

    def back_chunk(r, c):
        at = slice(c * LANES, (c + 1) * LANES)

        def body(i, carry):
            where = rows_of(r * step, i)
            gated = gx[c, pl.ds(pl.multiple_of(r * step + i * block + halo, 8), block), :]
            total = jnp.zeros((block, LANES), F32)
            for k in range(kernel_len):
                grad = gf[c, pl.ds(r * step + i * block + k, block), :]
                total = total + taps_ref[pl.ds(k, 1), at] * grad
                tacc[c, k] += (gated * grad).reshape(block // 8, 8, LANES).sum(axis=0)
            sigmoid = sg[where, at]
            value = vp[where, at].astype(F32)
            gb[c, where, :LANES] = (total * sigmoid).astype(BF)
            gb[c, where, LANES:] = (total * value * sigmoid * (1.0 - sigmoid)).astype(BF)
            return carry

        lax.fori_loop(0, per, body, 0)

    def partial_input(r, j):
        at = pl.ds(pl.multiple_of(j * cols_tp, cols_tp), cols_tp)
        total = right_product(gb[0, piece(r), :], ww[0, at, :])
        for c in range(1, halves):
            total = total + right_product(gb[c, piece(r), :], ww[c, at, :])
        return total

    x_copies, y_copies = [], []

    def near_block(r):
        xs[r, 0] = partial_input(r, t_cross).astype(BF)
        xs[r, 1] = partial_input(r, t_near).astype(BF)
        x_copies.append(send(xs.at[r], xr.at[r], x_send.at[r], x_recv.at[r], {"tp": t_near}))

    def far_block(r):
        far = partial_input(r, t_far)
        acc[piece(r), :] = partial_input(r, t)
        x_copies[r].wait_recv()
        ys[r] = (far + xr[r, 0].astype(F32)).astype(BF)
        y_copies.append(send(ys.at[r], yr.at[r], y_send.at[r], y_recv.at[r], {"tp": t_far}))
        acc[piece(r), :] += xr[r, 1].astype(F32)

    filtered_chunk(0)

    @pl.when(me > 0)
    def _():
        halo_f.start()

    for ks in pairs[1:]:
        send_mates(0, ks)
    todo = [(j, k) for j in range(1 + halves) for k in range(h - 1)]
    filtered_chunk(1)


    def far_steps(count):
        for _ in range(count):
            far_step(*todo.pop(0))

    for c in range(halves):
        back_chunk(0, c)
    near_block(0)
    early = group == 1
    for c in range(halves):
        for r in range(1, chunks):
            if c == 0 and r + 1 < chunks:
                filtered_chunk(r + 1)
            if c == 0 and r == chunks - 1:
                @pl.when(me < n - 1)
                def _():
                    halo_f.wait_recv()
            back_chunk(r, c)
            if c == 0 and r == 1:
                far_block(0)
                far_steps(1)
            if c == halves - 1:
                near_block(r)
                if r > 1:
                    far_block(r - 1)
                    far_steps(1)
        small[c, :kernel_len] = tacc[c].sum(axis=1)
        if c == halves - 1:
            small_copy = send(small.at[1 - inner], small_in, s_send.at[0], s_recv.at[0], {"sp": mate})
        make_others(1 + c, gb[c])
        mate_blocks(1 + c)
        if c == 0:
            far_steps(1)
    for c in range(halves):
        send_mates(1 + c, [h - 1])
    far_block(chunks - 1)

    loss_scale = 1.0 / math.sqrt(tokens * n)
    def input_chunk(r):
        y_copies[r].wait_recv()
        ig_ref[piece(r), :] = (acc[piece(r), :] + yr[r].astype(F32)).astype(BF)

    def weight_half(c):
        total = whole(1 + c)
        ws_ref[c] = total.T if aligned else total

    far_steps(len(todo) - h)
    late = todo.pop(0)
    far_step(*late, only=0 if early else None)
    small_copy.wait_recv()
    small_pair[...] = small[inner] + small_in[...]
    small_copies = [
        send(small_pair, small_all.at[outer], sa_send.at[k - 1], sa_recv.at[k - 1],
             {"sp": 2 * lax.rem(outer + k, h) + inner})
        for k in range(1, h)
    ]
    far_step(0, h - 1)
    total = whole(0)
    ps_ref[...] = total if aligned else total.T
    far_steps(len(todo) - 1)
    if early:
        far_step(*late, only=1)
    for copy in small_copies:
        copy.wait_recv()
    small_all[outer] = small_pair[...]
    total = small_all[0]
    for k in range(1, h):
        total = total + small_all[k]
    small_sum[inner] = total * loss_scale
    half_copy = send(
        small_sum.at[inner], small_sum.at[inner], sb_send.at[0], sb_recv.at[0], {"sp": mate}
    )
    for r in range(chunks - 1):
        input_chunk(r)
    far_steps(1)
    input_chunk(chunks - 1)
    for c in range(halves):
        far_step(1 + c, h - 1)
        weight_half(c)
    half_copy.wait_recv()
    sm_ref[...] = small_sum[...]

    @pl.when(me < n - 1)
    def _():
        halo_x.wait_send()

    @pl.when(me > 0)
    def _():
        halo_f.wait_send()

    for copies in mate_copies + far_copies + [list(found.values()) for found in low_copies]:
        sent.extend(copies)
    for copy in sent + x_copies + y_copies + small_copies + [small_copy, half_copy]:
        copy.wait_send()


def finish_kernel(
    ig_ref, ws_ref, ps_ref, sm_ref, ig_out, wv_out, wg_out, wp_out, taps_out, gain_out, shift_out,
    taps, gain, shift, sems,
):
    chans = ps_ref.shape[0]
    kernel_len = taps_out.shape[0]
    copies = []

    def store(src, dst):
        copies.append(pltpu.make_async_copy(src, dst, sems.at[len(copies)]))
        copies[-1].start()

    store(ig_ref, ig_out)
    store(ps_ref, wp_out)
    for c in range(chans // LANES):
        at = slice(c * LANES, (c + 1) * LANES)
        store(ws_ref.at[c, :, :LANES], wv_out.at[:, at])
        store(ws_ref.at[c, :, LANES:], wg_out.at[:, at])
        taps[:, at] = sm_ref[c, :kernel_len]
        gain[:, at] = sm_ref[c, kernel_len:kernel_len + 1]
        shift[:, at] = sm_ref[c, kernel_len + 1:kernel_len + 2]
    store(taps, taps_out)
    store(gain, gain_out)
    store(shift, shift_out)
    for copy in copies:
        copy.wait()


def shards(block_input, out_grad, w_value, w_gate, conv_taps, norm_gain, norm_shift, w_proj):
    n, n_tp = lax.axis_size("sp"), lax.axis_size("tp")
    tokens, width = block_input.shape
    chans = w_value.shape[1]
    kernel_len = conv_taps.shape[0]
    halves = chans // LANES
    halo = -(-(kernel_len - 1) // 8) * 8
    rows, cols, h, chunks = width // n, width // n_tp, n // 2, 4
    step = tokens // chunks
    smalls = (-(-(kernel_len + 2) // 8) * 8, LANES)
    pair, sums, lows = 2 * LANES, 1 + halves, max(h - 4, 1)
    part = (pair, rows) if rows % LANES == 0 else (rows, pair)
    anywhere = pl.BlockSpec(memory_space=pl.ANY)
    vmem = pl.BlockSpec(memory_space=pltpu.VMEM)
    dma = pltpu.SemaphoreType.DMA
    V = pltpu.VMEM
    shape = jax.ShapeDtypeStruct
    results = pl.pallas_call(
        functools.partial(main_kernel, n, n_tp, chans * n_tp, halo),
        out_shape=(
            shape((tokens, cols), BF), shape((halves, rows, pair), F32),
            shape((chans, rows), F32), shape((halves,) + smalls, F32),
        ),
        in_specs=[pl.BlockSpec(memory_space=pltpu.HBM)] * 8,
        out_specs=(vmem,) * 4,
        scratch_shapes=[
            V((tokens, width), BF), V((tokens, width), BF), V((halves, width, pair), BF),
            V((chans, width), BF), V((kernel_len, chans), F32), V((1, chans), F32), V((1, chans), F32),
            V((halves, halo + tokens, LANES), F32), V((tokens, chans), BF), V((tokens, chans), F32),
            V((halves, tokens, LANES), F32), V((halves, tokens, LANES), F32), V((halves, tokens, LANES), F32),
            V((halves, tokens + halo, LANES), F32), V((tokens, chans), F32), V((tokens, chans), BF),
            V((halves, tokens, pair), BF), V((sums, pair, tokens), BF), V((halves, kernel_len, 8, LANES), F32), V((2, tokens, LANES), F32),
            V((step, LANES), F32), V((2, chunks, 8, step), F32), V((2, chunks, n_tp - 1, 8, step), F32),
            V((sums, n) + part, BF), V((sums,) + part, F32), V((sums, h) + part, BF), V((sums, lows) + part, BF), V((sums, lows) + part, BF),
            V((sums, 3) + part, BF), V((sums, 4) + part, BF),
            V((chunks, 2, step, cols), BF), V((chunks, 2, step, cols), BF), V((chunks, step, cols), BF),
            V((chunks, step, cols), BF), V((tokens, cols), F32),
            V((halves,) + smalls, F32), V(smalls, F32), V(smalls, F32), V((h,) + smalls, F32),
            V((halves,) + smalls, F32),
            dma((2 * halves + chunks + 5,)), dma((2, chunks, n_tp - 1)), dma((2, chunks, n_tp - 1)),
            dma((1,)), dma((1,)), dma((1,)), dma((1,)),
            dma((sums, h)), dma((sums, h)), dma((sums, lows)), dma((sums, lows)), dma((sums, 3)), dma((sums, 4)),
            dma((chunks,)), dma((chunks,)), dma((chunks,)), dma((chunks,)), dma((1,)), dma((1,)),
            dma((h - 1,)), dma((h - 1,)), dma((1,)), dma((1,)),
        ],
        compiler_params=pltpu.CompilerParams(
            collective_id=0, has_side_effects=True, vmem_limit_bytes=52 * 1024 * 1024
        ),
        name="main",
    )(*[
        pltpu.with_memory_space_constraint(x, pltpu.HBM)
        for x in (
            block_input, out_grad, w_value, w_gate, w_proj, conv_taps,
            norm_gain.reshape(1, chans), norm_shift.reshape(1, chans),
        )
    ])
    outs = pl.pallas_call(
        finish_kernel,
        out_shape=(
            shape((tokens, cols), BF), shape((rows, chans), F32), shape((rows, chans), F32),
            shape((chans, rows), F32), shape((kernel_len, chans), F32), shape((1, chans), F32), shape((1, chans), F32),
        ),
        in_specs=[vmem] * 4,
        out_specs=(anywhere,) * 7,
        scratch_shapes=[
            V((kernel_len, chans), F32), V((1, chans), F32), V((1, chans), F32), dma((5 + 2 * halves,)),
        ],
        compiler_params=pltpu.CompilerParams(vmem_limit_bytes=4 * 1024 * 1024),
        name="finish",
    )(*results)
    return outs[:5] + (outs[5].reshape(chans), outs[6].reshape(chans))


def solution(mesh):
    return jax.shard_map(
        shards,
        mesh=mesh,
        in_specs=(
            P("sp", None),
            P("sp", None),
            P(None, "tp"),
            P(None, "tp"),
            P(None, "tp"),
            P("tp"),
            P("tp"),
            P("tp", None),
        ),
        out_specs=(
            P("sp", "tp"),
            P("sp", "tp"),
            P("sp", "tp"),
            P("tp", "sp"),
            P(None, "tp"),
            P("tp"),
            P("tp"),
        ),
        check_vma=False,
    )
```
